32 devices in a mesh: sp: 8 (over z, core), tp: 4 (over y, x).
Axes of the slice: x: 2, y: 2, z: 4, core: 2. Of those that a mesh axis runs over, the one named last changes fastest.
Arguments:
- residual_in: bfloat16 [2048, 2048], P('sp'), may hold values from -3 to 3
- mix_gain: float32 [2048], replicated, may hold values from 0.1 to 1.9
- pool_weight: bfloat16 [512, 2048], P(None, 'tp'), may hold values from -0.5 to 0.5
- pool_scale: float32 [2048], P('tp'), may hold values from 0.1 to 1.9
- ffn_gain: float32 [2048], replicated, may hold values from 0.1 to 1.9
- route_ids: int32 [2048, 2], P('sp'), may hold values from 0 to 7, all different within a row; in each aligned block of 64 rows (0 to 63, 64 to 127, ...) at most 32 rows name the same one
- route_weights: float32 [2048, 2], P('sp'), may hold values from 0.1 to 1
- gate_weight: bfloat16 [8, 2048, 3584], P('sp', None, 'tp'), may hold values from -0.125 to 0.125
- up_weight: bfloat16 [8, 2048, 3584], P('sp', None, 'tp'), may hold values from -0.125 to 0.125
- down_weight: bfloat16 [8, 3584, 2048], P('sp', 'tp'), may hold values from -0.09375 to 0.09375
Outputs:
- layer_out: bfloat16 [2048, 2048], P('sp')
The draws below stay inside these ranges and needn't reach their ends.
Inputs may be any that keep to these rules, and one draw needn't show every extreme that they name: `route_ids`: each row names 2 different experts; in each aligned block of 64 rows no expert is named by more than 32 rows, and some block has an expert named by exactly 32 rows.
All inputs are finite; a program needn't handle non-finite values.
Results may differ from the reference program's by a relative error of at most 0.0074.
Values may be sent and summed in bfloat16 or wider, within the bound.
A program may use at most 64 MiB of HBM per device.

```python
import math
import jax
import jax.numpy as jnp
import numpy as np
from jax import lax

D = 2048
GROUPS = 4
SPAN = 16
C = 512
FF_EXP = 3584
TOP_K = 2
EXPERTS = 8
ROWS = 64
CAP = 32
TOKENS = 2048
N_TP = 4


def level_of(rng, shape, split, smallest, top_value):
    def one(dim, parts):
        draws = jax.random.uniform(jax.random.fold_in(jax.random.fold_in(rng, 6), dim), (parts,), jnp.float32, smallest / len(split), top_value / len(split))
        return jnp.repeat(jnp.exp(draws), shape[dim] // parts).reshape((-1,) + (1,) * (len(shape) - dim - 1))

    factor_of = one(*split[0])
    for cut in split[1:]:
        factor_of = factor_of * one(*cut)
    return factor_of


def deal_out(key, own, number, rows, number_of, top, most, lean):
    sequence = jax.random.permutation(key, number_of)
    heavy_load, ordinary = shares(number_of, rows * top, most, lean, True), shares(number_of, rows * top, most, lean, False)
    places = jnp.arange(number_of)

    def named(sizes, offset_by):
        used = int((sizes > 0).sum())
        fixed = max(1, used // 4)
        passed = fixed + (places - fixed + offset_by * (used - fixed)) % max(1, number_of - fixed)
        return jnp.zeros((number_of,), jnp.int32).at[sequence[jnp.where(places < fixed, places, passed)]].set(jnp.asarray(sizes, jnp.int32))

    sizes = jnp.where(number % 4 == 0, named(heavy_load, number // 4), named(ordinary, number - number // 4 - 1))
    mixed = jax.random.permutation(jax.random.fold_in(own, 3), number_of)
    source_of, receiver = mixed[0:number_of // 2 * 2:2], mixed[1:number_of // 2 * 2:2]
    room = jnp.minimum(sizes[source_of] - 1, most - sizes[receiver]) // 2
    room = jnp.where((source_of == sequence[0]) | (receiver == sequence[0]) | (sizes[receiver] == 0), 0, jnp.maximum(room, 0))
    passed = jax.random.randint(jax.random.fold_in(own, 4), (number_of // 2,), 0, 1 << 20) % (room + 1)
    sizes = sizes.at[source_of].add(-passed).at[receiver].add(passed)
    items = jnp.searchsorted(jnp.cumsum(sizes), jnp.arange(rows * top), side="right").astype(jnp.int32)
    table = items.reshape(top, rows).T
    table = table[jax.random.permutation(jax.random.fold_in(own, 1), rows)]
    offset_by = jax.random.randint(jax.random.fold_in(own, 2), (rows, 1), 0, top)
    return jnp.take_along_axis(table, (jnp.arange(top)[None, :] + offset_by) % top, axis=1)


def shares(number_of, total, bound, lean, full):
    loads = [(1 << 20) // math.isqrt(standing ** lean) + 1 for standing in range(1, number_of + 1)]
    largest = bound if full else min(bound, max(-(-total // number_of), total * loads[0] // sum(loads)))
    least = 1 if total - largest >= number_of - 1 else 0
    counts, surplus = [largest] + [least] * (number_of - 1), total - largest - least * (number_of - 1)
    while surplus > 0:
        movable = [i for i in range(1, number_of) if counts[i] < largest] or [i for i in range(1, number_of) if counts[i] < bound]
        pool, remaining = sum([loads[i] for i in movable]), surplus
        for i in movable:
            extra = min(bound - counts[i], max(1, remaining * loads[i] // pool), surplus)
            counts[i] = counts[i] + extra
            surplus = surplus - extra
    return np.array(counts)


def gaussian(stream_key, shape, deviation, most, cuts=(), held_as=jnp.bfloat16):
    result = jax.random.normal(stream_key, shape, jnp.float32) * deviation
    if len(cuts) > 0:
        result = level_of(stream_key, shape, cuts, -0.22, 0.18) * result
    return jnp.clip(result, min=-most, max=most).astype(held_as)


def setup_inputs(seed: int = 0) -> dict:
    streams_of = jax.random.split(jax.random.key(seed), 11)
    residual_in = gaussian(streams_of[0], (TOKENS, D), 0.5, 3.0, ((0, 8),))
    mix_gain = jnp.clip(1.0 + 0.18 * jax.random.normal(streams_of[1], (D,), jnp.float32), 0.1, 1.9)
    pool_weight = gaussian(streams_of[2], (C, D), (C // 4) ** -0.5, 0.5, ((1, 4),))
    pool_scale = jnp.clip(1.0 + 0.18 * jax.random.normal(streams_of[3], (D,), jnp.float32), 0.1, 1.9)
    ffn_gain = jnp.clip(1.0 + 0.18 * jax.random.normal(streams_of[4], (D,), jnp.float32), 0.1, 1.9)
    route_ids_keys = jax.random.split(jax.random.fold_in(streams_of[5], 1), TOKENS // ROWS)
    route_ids_turns = jax.random.permutation(jax.random.fold_in(streams_of[5], 3), TOKENS // ROWS)
    route_ids = jax.vmap(lambda own, number: deal_out(jax.random.fold_in(streams_of[5], 2), own, number, ROWS, EXPERTS, TOP_K, CAP, 2))(route_ids_keys, route_ids_turns).reshape((TOKENS, TOP_K))
    route_weights = jnp.clip(jnp.exp(math.log(1.0) - 2.3025851 * jax.random.uniform(streams_of[6], (TOKENS, TOP_K), jnp.float32) ** level_of(streams_of[6], (TOKENS, TOP_K), ((0, 8),), -0.2, 0.2)), 0.1, 1.0)
    gate_weight = gaussian(streams_of[7], (EXPERTS, D, FF_EXP), D ** -0.5, 0.125, ((0, 8), (2, 4)))
    up_weight = gaussian(streams_of[8], (EXPERTS, D, FF_EXP), D ** -0.5, 0.125, ((0, 8), (2, 4)))
    down_weight = gaussian(streams_of[9], (EXPERTS, FF_EXP, D), FF_EXP ** -0.5, 0.09375, ((0, 8), (1, 4)))
    return {"residual_in": residual_in, "mix_gain": mix_gain, "pool_weight": pool_weight, "pool_scale": pool_scale, "ffn_gain": ffn_gain, "route_ids": route_ids, "route_weights": route_weights, "gate_weight": gate_weight, "up_weight": up_weight, "down_weight": down_weight}


EPS = 1e-06

def rms_scale(values, gain):
    return values * lax.rsqrt(lax.optimization_barrier(jnp.mean(values * values, axis=-1, keepdims=True)) + EPS) * gain

def reference(residual_in, mix_gain, pool_weight, pool_scale, ffn_gain, route_ids, route_weights, gate_weight, up_weight, down_weight):
    stream = residual_in.astype(jnp.float32)
    normed_in = rms_scale(stream, mix_gain).astype(jnp.bfloat16)
    shifted_in = jnp.concatenate([jnp.zeros((SPAN, D), jnp.bfloat16), normed_in], axis=0).astype(jnp.float32)
    position = jnp.arange(TOKENS, dtype=jnp.int32)
    pieces = []
    for group_index in range(GROUPS):
        window = 2 ** (group_index + 1)
        first = group_index * C
        window_sum = jnp.zeros((TOKENS, C), jnp.float32)
        for offset in range(window):
            window_sum = window_sum + shifted_in[SPAN - offset:SPAN - offset + TOKENS, first:first + C]
        divisor = jnp.minimum(position + 1, window).astype(jnp.float32)
        pieces.append(window_sum / divisor[:, None] - shifted_in[SPAN:, first:first + C])
    pooled = jnp.concatenate(pieces, axis=1).astype(jnp.bfloat16)
    mapped = jnp.concatenate([jnp.dot(pooled[:, g * C:(g + 1) * C], pool_weight[:, g * C:(g + 1) * C], preferred_element_type=jnp.float32) for g in range(GROUPS)], axis=1)
    mixer_out = (mapped * pool_scale).astype(jnp.bfloat16)
    after_mixer = (stream + mixer_out.astype(jnp.float32)).astype(jnp.bfloat16)
    normed = rms_scale(after_mixer.astype(jnp.float32), ffn_gain).astype(jnp.bfloat16)
    block_count = TOKENS // ROWS
    grouped = route_ids.reshape(block_count, ROWS * TOP_K)
    matches = (grouped[:, :, None] == jnp.arange(EXPERTS, dtype=jnp.int32)[None, None, :]).astype(jnp.int32)
    before = jnp.cumsum(matches, axis=1) - matches
    slot_of = lax.optimization_barrier(jnp.sum(before * matches, axis=-1))
    target = grouped * (block_count * CAP) + jnp.arange(block_count, dtype=jnp.int32)[:, None] * CAP + slot_of
    target = target.reshape(-1).astype(jnp.int32)
    source = (jnp.arange(TOKENS * TOP_K, dtype=jnp.int32) // TOP_K).astype(jnp.int32)
    holder = jnp.zeros((EXPERTS * block_count * CAP,), jnp.int32).at[target].set(source)
    share = FF_EXP // N_TP

    def run_expert(operands):
        indices, gate_matrix, up_matrix, down_matrix = operands
        chosen = normed[indices]
        gate_part = jnp.dot(chosen, gate_matrix, preferred_element_type=jnp.float32)
        up_part = jnp.dot(chosen, up_matrix, preferred_element_type=jnp.float32)
        hidden = (jax.nn.silu(gate_part) * up_part).astype(jnp.bfloat16)
        total = jnp.zeros((indices.shape[0], D), jnp.float32)
        for piece in range(N_TP):
            partial_value = jnp.dot(hidden[:, piece * share:(piece + 1) * share], down_matrix[piece * share:(piece + 1) * share], preferred_element_type=jnp.float32)
            total = total + partial_value.astype(jnp.bfloat16).astype(jnp.float32)
        return total.astype(jnp.bfloat16)
    outputs = lax.map(run_expert, (holder.reshape(EXPERTS, block_count * CAP), gate_weight, up_weight, down_weight))
    picked = outputs.reshape(-1, D)[target].astype(jnp.float32).reshape(TOKENS, TOP_K, D)
    expert_mix = lax.optimization_barrier(jnp.sum(route_weights[:, :, None] * picked, axis=1))
    return (after_mixer.astype(jnp.float32) + expert_mix).astype(jnp.bfloat16)
```

```python
import functools

import jax
import jax.numpy as jnp
from jax import lax
from jax.experimental import pallas as pl
from jax.experimental.pallas import tpu as pltpu
from jax.sharding import PartitionSpec as P

GROUPS = 4
SPAN = 16
TOP_K = 2
CORES = 2
SIDE = 2
LANES = 128
EPS = 1e-06
MESH = pl.DeviceIdType.MESH
ZU, ZD, X, Y, DX, DY, FX, FY, FDX, FDY = range(10)

def from_behind(value, axis, steps):
    count = lax.axis_size(axis)
    first, last = (max(0, -steps), min(count, count - steps))
    return lax.ppermute(value, axis, [(source, source + steps) for source in range(first, last)])


def rms_scale(values, gain):
    return values * lax.rsqrt(jnp.mean(values * values, axis=-1, keepdims=True) + EPS) * gain


def slot_table(chosen_ids, experts, capacity):
    flat_ids = chosen_ids.reshape(-1)
    matches = (flat_ids[:, None] == jnp.arange(experts, dtype=jnp.int32)[None, :]).astype(jnp.int32)
    before = jnp.cumsum(matches, axis=0) - matches
    slot_of = jnp.sum(before * matches, axis=1)
    target = flat_ids * capacity + slot_of
    return (target[:, None] == jnp.arange(experts * capacity, dtype=jnp.int32)[None, :]).astype(
        jnp.float32
    )


def shards_any(
    residual_in,
    mix_gain,
    pool_weight,
    pool_scale,
    ffn_gain,
    route_ids,
    route_weights,
    gate_weight,
    up_weight,
    down_weight,
):
    tp_count = lax.axis_size("tp")
    sp_count = lax.axis_size("sp")
    tp_index = lax.axis_index("tp")
    tok_count, width = residual_in.shape
    group_width = width // GROUPS
    col_count = pool_weight.shape[1]
    row_count = tok_count // tp_count
    capacity = 2 * TOP_K * row_count // sp_count
    group_index = tp_index * col_count // group_width
    window = jnp.power(2, group_index + 1)
    stream = residual_in.astype(jnp.float32)
    inverse = lax.rsqrt(jnp.mean(stream * stream, axis=-1, keepdims=True) + EPS)
    stream_group = lax.dynamic_slice_in_dim(stream, group_index * group_width, group_width, 1)
    gain_group = lax.dynamic_slice_in_dim(mix_gain, group_index * group_width, group_width, 0)
    normed_group = (stream_group * inverse * gain_group).astype(jnp.bfloat16)
    rim_rows = from_behind(normed_group[tok_count - SPAN :], "sp", 1)
    extended = jnp.concatenate([rim_rows, normed_group], axis=0).astype(jnp.float32)
    window_sum = jnp.zeros((tok_count, group_width), jnp.float32)
    for offset in range(SPAN):
        window_sum = window_sum + jnp.where(
            offset < window, extended[SPAN - offset : SPAN - offset + tok_count], 0.0
        )
    position = lax.axis_index("sp") * tok_count + jnp.arange(tok_count, dtype=jnp.int32)
    divisor = jnp.minimum(position + 1, window).astype(jnp.float32)
    pooled = (window_sum / divisor[:, None] - extended[SPAN:]).astype(jnp.bfloat16)
    mixed = (jnp.dot(pooled, pool_weight, preferred_element_type=jnp.float32) * pool_scale).astype(
        jnp.bfloat16
    )
    stream_own = lax.dynamic_slice_in_dim(stream, tp_index * row_count, row_count, 0)
    mixed_own = lax.all_to_all(mixed, "tp", split_axis=0, concat_axis=1, tiled=True)
    after_own = (stream_own + mixed_own.astype(jnp.float32)).astype(jnp.bfloat16)
    normed_own = rms_scale(after_own.astype(jnp.float32), ffn_gain).astype(jnp.bfloat16)
    ids_own = lax.dynamic_slice_in_dim(route_ids, tp_index * row_count, row_count, 0)
    table_own = slot_table(ids_own, sp_count, capacity)
    repeated = jnp.repeat(normed_own, TOP_K, axis=0)
    outgoing = lax.dot_general(
        table_own.astype(jnp.bfloat16),
        repeated,
        (((0,), (0,)), ((), ())),
        preferred_element_type=jnp.float32,
    )
    outgoing = outgoing.astype(jnp.bfloat16).reshape(sp_count, capacity, width)
    arrived = lax.all_to_all(outgoing, "sp", split_axis=0, concat_axis=0, tiled=True)
    piece = lax.all_gather(arrived, "tp", axis=0, tiled=True)
    flat_rows = piece.reshape(-1, width)
    gate_part = jnp.dot(flat_rows, gate_weight[0], preferred_element_type=jnp.float32)
    up_part = jnp.dot(flat_rows, up_weight[0], preferred_element_type=jnp.float32)
    hidden = (jax.nn.silu(gate_part) * up_part).astype(jnp.bfloat16)
    hidden_all = hidden.reshape(piece.shape[0], piece.shape[1], hidden.shape[1])
    hidden_flat = hidden_all.reshape(-1, hidden_all.shape[-1])
    term = jnp.dot(hidden_flat, down_weight[0], preferred_element_type=jnp.float32)
    summed = lax.psum_scatter(
        term.astype(jnp.bfloat16).astype(jnp.float32).astype(jnp.bfloat16),
        "tp",
        scatter_dimension=0,
        tiled=True,
    )
    expert_out = summed.reshape(sp_count, capacity, width)
    returned_rows = lax.all_to_all(expert_out, "sp", split_axis=0, concat_axis=0, tiled=True)
    weights_own = lax.dynamic_slice_in_dim(route_weights, tp_index * row_count, row_count, 0)
    weight_table = jnp.einsum(
        "rk,rkc->rc", weights_own, table_own.reshape(row_count, TOP_K, sp_count * capacity)
    )
    expert_mix = jnp.dot(
        weight_table,
        returned_rows.reshape(-1, width).astype(jnp.float32),
        precision=lax.Precision.HIGHEST,
    )
    out_own = (after_own.astype(jnp.float32) + expert_mix).astype(jnp.bfloat16)
    return lax.all_gather(out_own, "tp", axis=0, tiled=True)


class Place:
    def __init__(self, send_sem, recv_sem):
        self.sp, self.tp = lax.axis_index("sp"), lax.axis_index("tp")
        self.levels = lax.axis_size("sp") // CORES
        self.z, self.c = self.sp // CORES, self.sp % CORES
        y, x = self.tp // SIDE, self.tp % SIDE
        self.tx = y * SIDE + (1 - x)
        self.ty = (1 - y) * SIDE + x
        self.td = (1 - y) * SIDE + (1 - x)
        self.send_sem, self.recv_sem = send_sem, recv_sem
        partner = self.z * CORES + (1 - self.c)
        self.partner = (partner, self.tp)
        self.to = {
            ZU: (self.sp + CORES, self.tp),
            ZD: (self.sp - CORES, self.tp),
            X: (self.sp, self.tx),
            Y: (self.sp, self.ty),
        }
        for kind, base in ((DX, X), (DY, Y), (FX, X), (FY, Y), (FDX, X), (FDY, Y)):
            self.to[kind] = self.to[base]

    def copy(self, kind, index, src, dst):
        return pltpu.make_async_remote_copy(
            src_ref=src,
            dst_ref=dst,
            send_sem=self.send_sem.at[kind, index],
            recv_sem=self.recv_sem.at[kind, index],
            device_id=self.to[kind],
            device_id_type=MESH,
        )

    def exists(self, offset):
        level = self.z + offset
        return (level >= 0) & (level < self.levels)

    def offsets(self):
        order = [0]
        for distance in range(1, self.levels):
            order += [-distance, distance]
        return order


def greet(place, everyone):
    barrier = pltpu.get_barrier_semaphore()

    def hello(target):
        pl.semaphore_signal(barrier, inc=1, device_id=target, device_id_type=MESH)

    hello(place.to[X])
    hello(place.to[Y])
    if everyone:
        count = lax.axis_size("sp")
        for step in range(1, count):
            hello((lax.rem(place.sp + step, count), place.tp))
        pl.semaphore_wait(barrier, count + 1)
    else:
        hello(place.partner)
        for step in range(1, place.levels):
            hello((lax.rem(place.z + step, place.levels) * CORES + place.c, place.tp))
        pl.semaphore_wait(barrier, place.levels + 2)


def gather_kernel(
    own_ref, meta_ref, result_ref, meta_out,
    out_ref, send_sem, recv_sem, p_send, p_recv, m_send, m_recv, l_sem, o_sem,
):
    place = Place(send_sem, recv_sem)
    rows, cols = own_ref.shape
    half = rows // 2
    z, c, tp = place.z, place.c, place.tp
    sp_count = lax.axis_size("sp")
    tiles = SIDE * SIDE

    def block(level, core, tile, first=0, count=rows):
        start = pl.multiple_of((level * CORES + core) * rows + first, half)
        return out_ref.at[pl.ds(start, count), pl.ds(pl.multiple_of(tile * cols, cols), cols)]

    def put_out(level, tile, core):
        start = pl.multiple_of((level * CORES + core) * rows, rows)
        lanes = pl.ds(pl.multiple_of(tile * cols, cols), cols)
        return pltpu.make_async_copy(
            block(level, core, tile),
            result_ref.at[pl.ds(start, rows), lanes],
            o_sem.at[level, tile, core],
        )

    def pair_copy(level, tile, core):
        ref = block(level, core, tile)
        return pltpu.make_async_remote_copy(
            src_ref=ref,
            dst_ref=ref,
            send_sem=p_send.at[level, tile],
            recv_sem=p_recv.at[level, tile],
            device_id=place.partner,
            device_id_type=MESH,
        )

    def meta_copy(step):
        target = lax.rem(place.sp + step, sp_count)
        return pltpu.make_async_remote_copy(
            src_ref=meta_ref,
            dst_ref=meta_out.at[place.sp],
            send_sem=m_send.at[step],
            recv_sem=m_recv.at[step],
            device_id=(target, tp),
            device_id_type=MESH,
        )

    local = pltpu.make_async_copy(own_ref, block(z, c, tp), l_sem.at[0])
    local.start()
    local_meta = pltpu.make_async_copy(meta_ref, meta_out.at[place.sp], l_sem.at[1])
    local_meta.start()
    local.wait()
    local_meta.wait()
    greet(place, True)

    def whole(kind, level, tile):
        ref = block(level, c, tile)
        return place.copy(kind, level, ref, ref)

    def part(kind, level, tile):
        ref = block(level, c, tile, 0 if kind == DY else half, half)
        return place.copy(kind, level, ref, ref)

    def first(offset):
        level = z + offset
        if offset < 0:
            whole(ZU, level, tp).wait_recv()
        if offset > 0:
            whole(ZD, level, tp).wait_recv()
        if offset <= 0:
            pl.when(place.exists(1))(lambda: whole(ZU, level, tp).start())
        if offset >= 0:
            pl.when(place.exists(-1))(lambda: whole(ZD, level, tp).start())
        whole(X, level, tp).start()
        whole(Y, level, tp).start()
        pair_copy(level, tp, c).start()
        put_out(level, tp, c).start()

    def second(offset):
        level = z + offset
        whole(X, level, place.tx).wait_recv()
        part(DY, level, place.tx).start()
        pair_copy(level, place.tx, c).start()
        put_out(level, place.tx, c).start()
        whole(Y, level, place.ty).wait_recv()
        part(DX, level, place.ty).start()
        pair_copy(level, place.ty, c).start()
        put_out(level, place.ty, c).start()

    def third(offset):
        level = z + offset
        part(DY, level, place.td).wait_recv()
        part(DX, level, place.td).wait_recv()
        pair_copy(level, place.td, c).start()
        put_out(level, place.td, c).start()

    order = place.offsets()
    stages = ((first, 0), (second, 1), (third, 2))
    for step in range(place.levels + 2):
        for stage, lag in stages:
            for offset in order:
                if abs(offset) == step - lag:
                    pl.when(place.exists(offset))(functools.partial(stage, offset))
        if step == 0:
            for hop in range(1, sp_count):
                meta_copy(hop).start()

    pairs = [(level, tile) for level in range(place.levels) for tile in range(tiles)]
    for level, tile in pairs:
        pair_copy(level, tile, 1 - c).wait_recv()
        put_out(level, tile, 1 - c).start()
    for hop in range(1, sp_count):
        meta_copy(hop).wait_send()
        meta_copy(hop).wait_recv()

    def sent(offset):
        level = z + offset
        if offset <= 0:
            pl.when(place.exists(1))(lambda: whole(ZU, level, tp).wait_send())
        if offset >= 0:
            pl.when(place.exists(-1))(lambda: whole(ZD, level, tp).wait_send())
        whole(X, level, tp).wait_send()
        whole(Y, level, tp).wait_send()
        part(DY, level, place.tx).wait_send()
        part(DX, level, place.ty).wait_send()

    for offset in order:
        pl.when(place.exists(offset))(functools.partial(sent, offset))
    for level, tile in pairs:
        pair_copy(level, tile, c).wait_send()
        put_out(level, tile, c).wait()
        put_out(level, tile, 1 - c).wait()


def gather_all(own, meta, sp_count, tp_count):
    rows, cols = own.shape
    levels = sp_count // CORES
    vmem = pl.BlockSpec(memory_space=pltpu.VMEM)
    return pl.pallas_call(
        gather_kernel,
        out_shape=(
            jax.ShapeDtypeStruct((sp_count * rows, tp_count * cols), own.dtype),
            jax.ShapeDtypeStruct((sp_count,) + meta.shape, meta.dtype),
        ),
        in_specs=[vmem, vmem],
        out_specs=(pl.BlockSpec(memory_space=pl.ANY), vmem),
        scratch_shapes=[
            pltpu.VMEM((sp_count * rows, tp_count * cols), own.dtype),
            pltpu.SemaphoreType.DMA((6, levels)),
            pltpu.SemaphoreType.DMA((6, levels)),
            pltpu.SemaphoreType.DMA((levels, tp_count)),
            pltpu.SemaphoreType.DMA((levels, tp_count)),
            pltpu.SemaphoreType.DMA((sp_count,)),
            pltpu.SemaphoreType.DMA((sp_count,)),
            pltpu.SemaphoreType.DMA((2,)),
            pltpu.SemaphoreType.DMA((levels, tp_count, CORES)),
        ],
        compiler_params=pltpu.CompilerParams(collective_id=0, has_side_effects=True),
        name="gather_all",
    )(own, meta)


def level_order(place):
    everywhere = range(place.levels)
    orders = []
    for z in everywhere:
        offsets = [offset for offset in place.offsets()[::-1] if 0 <= z + offset < place.levels]
        orders.append([z + offset for offset in offsets])
    steps = []
    for index in everywhere:
        level = jnp.int32(orders[0][index])
        for z in everywhere[1:]:
            level = jnp.where(place.z == z, orders[z][index], level)
        steps.append(level)
    return steps


def experts_kernel(
    rows_ref, slot_ref, weight_ref, gain_ref, gate_ref, up_ref, down_ref, after_ref, out_ref,
    held, gu, dn, picked, hid, spread, scale, parts,
    r_pair, s_diag, r_ydiag, r_xdiag, s_x, s_y, r_x, r_y, s_z, r_z,
    send_sem, recv_sem, p_send, p_recv, z_send, z_recv, h_sem, w_sem,
):
    place = Place(send_sem, recv_sem)
    rows, cols = after_ref.shape
    width = rows_ref.shape[1]
    slots = spread.shape[2]
    half = rows // 2
    z, c, tp = place.z, place.c, place.tp
    chunk = 32
    pieces, _, pair_lanes = gu.shape
    lanes_each = pair_lanes // 2
    order = level_order(place)
    wide = 256

    def held_copy(level):
        at = pl.ds(pl.multiple_of(level * CORES * rows, CORES * rows), CORES * rows)
        return pltpu.make_async_copy(rows_ref.at[at], held.at[level], h_sem.at[level])

    def gate_copy(piece, side):
        source = (gate_ref, up_ref)[side]
        return pltpu.make_async_copy(
            source.at[0, :, pl.ds(piece * lanes_each, lanes_each)],
            gu.at[piece, :, pl.ds(side * lanes_each, lanes_each)],
            w_sem.at[piece, side],
        )

    down_copy = pltpu.make_async_copy(down_ref.at[0], dn, w_sem.at[pieces, 0])

    held_copy(order[0]).start()
    for piece in range(pieces):
        gate_copy(piece, 0).start()
        gate_copy(piece, 1).start()
    down_copy.start()
    for level in order[1:]:
        held_copy(level).start()
    greet(place, False)

    def pair_copy(level):
        return pltpu.make_async_remote_copy(
            src_ref=parts.at[level, 1 - c],
            dst_ref=r_pair.at[level],
            send_sem=p_send.at[level],
            recv_sem=p_recv.at[level],
            device_id=place.partner,
            device_id_type=MESH,
        )

    def pick(level):
        held_copy(level).wait()
        for b in range(CORES):
            slot = slot_ref[level * CORES + b]
            weight = weight_ref[level * CORES + b]
            at = lax.broadcasted_iota(jnp.int32, (slots, rows), 0).astype(jnp.float32)
            chosen = at == slot
            table = jnp.where(chosen, 1.0, 0.0)
            scale[b] = jnp.sum(jnp.where(chosen, weight, 0.0), axis=1, keepdims=True)
            spread[b] = table.T.astype(jnp.bfloat16)
            table = table.astype(jnp.bfloat16)
            squares = jnp.zeros((slots, 1), jnp.float32)
            into = slice(b * slots, (b + 1) * slots)
            for start in range(0, width, wide):
                lanes = slice(start, start + wide)
                value = jnp.dot(
                    table,
                    held[level, b * rows : (b + 1) * rows, lanes],
                    preferred_element_type=jnp.float32,
                )
                squares = squares + jnp.sum(value * value, axis=1, keepdims=True)
                picked[into, lanes] = value.astype(jnp.bfloat16)
            inverse = lax.rsqrt(squares / width + EPS)
            for start in range(0, width, wide):
                lanes = slice(start, start + wide)
                value = picked[into, lanes].astype(jnp.float32) * inverse * gain_ref[:, lanes]
                picked[into, lanes] = value.astype(jnp.bfloat16)

    def grow(first_time):
        for piece in range(pieces):
            if first_time:
                gate_copy(piece, 0).wait()
                gate_copy(piece, 1).wait()
            both = jnp.dot(picked[...], gu[piece], preferred_element_type=jnp.float32)
            gate, up = both[:, :lanes_each], both[:, lanes_each:]
            lanes = slice(piece * lanes_each, (piece + 1) * lanes_each)
            hid[:, lanes] = (jax.nn.silu(gate) * up).astype(jnp.bfloat16)

    def shrink(level, first_time):
        if first_time:
            down_copy.wait()
        for start in range(0, width, 2 * wide):
            lanes = slice(start, start + 2 * wide)
            term = jnp.dot(hid[...], dn[:, lanes], preferred_element_type=jnp.float32)
            for b in range(CORES):
                scaled = (term[b * slots : (b + 1) * slots] * scale[b]).astype(jnp.bfloat16)
                value = jnp.dot(spread[b], scaled, preferred_element_type=jnp.float32)
                parts[level, b, :, lanes] = value.astype(jnp.bfloat16)
        pair_copy(level).start()

    def summed(level, tile, row, count=chunk):
        at = pl.ds(pl.multiple_of(row, chunk), count)
        lanes = pl.ds(pl.multiple_of(tile * cols, cols), cols)
        mine = parts[level, c, at, lanes].astype(jnp.float32)
        return mine + r_pair[level, at, lanes].astype(jnp.float32)

    def over(first, last, body):
        def step(index, carry):
            body(pl.multiple_of(first + index * chunk, chunk))
            return carry

        lax.fori_loop(0, (last - first) // chunk, step, 0)

    def diag(kind, level):
        if kind == DY:
            return place.copy(kind, level, s_diag.at[level, pl.ds(0, half)], r_ydiag.at[level])
        return place.copy(kind, level, s_diag.at[level, pl.ds(half, half)], r_xdiag.at[level])

    def side(kind, level):
        if kind == X:
            return place.copy(kind, level, s_x.at[level], r_x.at[level])
        return place.copy(kind, level, s_y.at[level], r_y.at[level])

    def line(level):
        return pltpu.make_async_remote_copy(
            src_ref=s_z.at[level],
            dst_ref=r_z.at[z],
            send_sem=z_send.at[level],
            recv_sem=z_recv.at[z],
            device_id=(level * CORES + c, tp),
            device_id_type=MESH,
        )

    def line_arrival(level):
        return pltpu.make_async_remote_copy(
            src_ref=s_z.at[level],
            dst_ref=r_z.at[level],
            send_sem=z_send.at[level],
            recv_sem=z_recv.at[level],
            device_id=(level * CORES + c, tp),
            device_id_type=MESH,
        )

    def first(level):
        pair_copy(level).wait_recv()

        def body(row):
            s_diag[level, pl.ds(row, chunk)] = summed(level, place.td, row).astype(jnp.bfloat16)

        over(0, half, body)
        diag(DY, level).start()
        over(half, rows, body)
        diag(DX, level).start()

    def second(level):
        def plain(buffer, tile):
            def body(row):
                buffer[level, pl.ds(row, chunk)] = summed(level, tile, row).astype(jnp.bfloat16)

            return body

        def joined(buffer, tile, arrived, base):
            def body(row):
                other = arrived[level, pl.ds(pl.multiple_of(row - base, chunk), chunk)]
                total = summed(level, tile, row) + other.astype(jnp.float32)
                buffer[level, pl.ds(row, chunk)] = total.astype(jnp.bfloat16)

            return body

        over(half, rows, plain(s_x, place.tx))
        over(0, half, plain(s_y, place.ty))
        diag(DY, level).wait_recv()
        over(0, half, joined(s_x, place.tx, r_ydiag, 0))
        side(X, level).start()
        diag(DX, level).wait_recv()
        over(half, rows, joined(s_y, place.ty, r_xdiag, half))
        side(Y, level).start()

    def third(level):
        side(X, level).wait_recv()
        side(Y, level).wait_recv()

        def body(row):
            at = pl.ds(row, chunk)
            total = summed(level, tp, row)
            total = total + r_x[level, at].astype(jnp.float32) + r_y[level, at].astype(jnp.float32)
            s_z[level, at] = total.astype(jnp.bfloat16)

        over(0, rows, body)
        line(level).start()

    def finish(level):
        side(X, level).wait_recv()
        side(Y, level).wait_recv()
        for other in order[:-1]:
            line_arrival(other).wait_recv()

        def body(row):
            at = pl.ds(row, chunk)
            total = summed(level, tp, row)
            total = total + r_x[level, at].astype(jnp.float32) + r_y[level, at].astype(jnp.float32)
            for other in order[:-1]:
                total = total + r_z[other, at].astype(jnp.float32)
            total = total + after_ref[at].astype(jnp.float32)
            lanes = pl.ds(pl.multiple_of(tp * cols, cols), cols)
            out_ref[at, lanes] = total.astype(jnp.bfloat16)

        over(0, rows, body)

    last = place.levels - 1
    for step in range(place.levels + 1):
        if step <= last:
            pick(order[step])
        if step >= 1:
            first(order[step - 1])
        if 3 <= step <= last:
            third(order[step - 3])
        if step <= last:
            grow(step == 0)
        if step >= 1:
            second(order[step - 1])
        if step <= last:
            shrink(order[step], step == 0)
    for step in range(max(0, last - 2), last):
        third(order[step])
    finish(order[last])

    def final(kind, tile):
        start, count = {FX: (0, rows), FY: (0, rows), FDY: (0, half), FDX: (half, half)}[kind]
        ref = out_ref.at[pl.ds(start, count), pl.ds(pl.multiple_of(tile * cols, cols), cols)]
        return place.copy(kind, 0, ref, ref)

    final(FX, tp).start()
    final(FY, tp).start()

    def sent(level, own):
        pair_copy(level).wait_send()
        for kind in (DX, DY):
            diag(kind, level).wait_send()
        for kind in (X, Y):
            side(kind, level).wait_send()
        if not own:
            line(level).wait_send()

    final(FX, place.tx).wait_recv()
    final(FDY, place.tx).start()
    final(FY, place.ty).wait_recv()
    final(FDX, place.ty).start()
    for step, level in enumerate(order):
        sent(level, step == last)
    final(FDY, place.td).wait_recv()
    final(FDX, place.td).wait_recv()
    final(FX, tp).wait_send()
    final(FY, tp).wait_send()
    final(FDY, place.tx).wait_send()
    final(FDX, place.ty).wait_send()


def experts_all(after_all, slot_of, weight, gain, gate, up, down, after, capacity, sp_count, tp_count):
    rows, cols = after.shape
    width = tp_count * cols
    hidden = gate.shape[2]
    levels = sp_count // CORES
    slots = capacity * tp_count
    vmem = pl.BlockSpec(memory_space=pltpu.VMEM)
    hbm = pl.BlockSpec(memory_space=pl.ANY)
    whole = pltpu.VMEM((levels, rows, cols), jnp.bfloat16)
    halved = pltpu.VMEM((levels, rows // 2, cols), jnp.bfloat16)
    pieces = hidden // LANES
    return pl.pallas_call(
        experts_kernel,
        out_shape=jax.ShapeDtypeStruct((rows, width), after.dtype),
        in_specs=[hbm, vmem, vmem, vmem, hbm, hbm, hbm, vmem],
        out_specs=vmem,
        scratch_shapes=[
            pltpu.VMEM((levels, CORES * rows, width), jnp.bfloat16),
            pltpu.VMEM((pieces, width, 2 * LANES), jnp.bfloat16),
            pltpu.VMEM((hidden, width), jnp.bfloat16),
            pltpu.VMEM((CORES * slots, width), jnp.bfloat16),
            pltpu.VMEM((CORES * slots, hidden), jnp.bfloat16),
            pltpu.VMEM((CORES, rows, slots), jnp.bfloat16),
            pltpu.VMEM((CORES, slots, 1), jnp.float32),
            pltpu.VMEM((levels, CORES, rows, width), jnp.bfloat16),
            pltpu.VMEM((levels, rows, width), jnp.bfloat16),
            whole, halved, halved, whole, whole, whole, whole, whole, whole,
            pltpu.SemaphoreType.DMA((10, levels)),
            pltpu.SemaphoreType.DMA((10, levels)),
            pltpu.SemaphoreType.DMA((levels,)),
            pltpu.SemaphoreType.DMA((levels,)),
            pltpu.SemaphoreType.DMA((levels,)),
            pltpu.SemaphoreType.DMA((levels,)),
            pltpu.SemaphoreType.DMA((levels,)),
            pltpu.SemaphoreType.DMA((pieces + 1, 2)),
        ],
        compiler_params=pltpu.CompilerParams(
            collective_id=1, has_side_effects=True, vmem_limit_bytes=62 * 1024 * 1024
        ),
        name="experts_all",
    )(after_all, slot_of, weight, gain, gate, up, down, after)


def shards(
    residual_in,
    mix_gain,
    pool_weight,
    pool_scale,
    ffn_gain,
    route_ids,
    route_weights,
    gate_weight,
    up_weight,
    down_weight,
):
    tp_count = lax.axis_size("tp")
    sp_count = lax.axis_size("sp")
    tp_index = lax.axis_index("tp")
    tok_count, width = residual_in.shape
    group_width = width // GROUPS
    col_count = pool_weight.shape[1]
    block_rows = tok_count // tp_count
    capacity = 2 * TOP_K * block_rows // sp_count
    group_index = tp_index * col_count // group_width
    window = jnp.power(2, group_index + 1)
    stream = residual_in.astype(jnp.float32)
    inverse = lax.rsqrt(jnp.mean(stream * stream, axis=-1, keepdims=True) + EPS)
    stream_group = lax.dynamic_slice_in_dim(residual_in, group_index * group_width, group_width, 1)
    stream_group = stream_group.astype(jnp.float32)
    gain_group = lax.dynamic_slice_in_dim(mix_gain, group_index * group_width, group_width, 0)
    normed_group = (stream_group * inverse * gain_group).astype(jnp.bfloat16)
    rim_rows = from_behind(normed_group[tok_count - SPAN :], "sp", 1)
    extended = jnp.concatenate([rim_rows, normed_group], axis=0).astype(jnp.float32)
    window_sum = jnp.zeros((tok_count, group_width), jnp.float32)
    for offset in range(SPAN):
        window_sum = window_sum + jnp.where(
            offset < window, extended[SPAN - offset : SPAN - offset + tok_count], 0.0
        )
    position = lax.axis_index("sp") * tok_count + jnp.arange(tok_count, dtype=jnp.int32)
    divisor = jnp.minimum(position + 1, window).astype(jnp.float32)
    pooled = (window_sum / divisor[:, None] - extended[SPAN:]).astype(jnp.bfloat16)
    mixed = (jnp.dot(pooled, pool_weight, preferred_element_type=jnp.float32) * pool_scale).astype(
        jnp.bfloat16
    )
    stream_own = lax.dynamic_slice_in_dim(residual_in, tp_index * col_count, col_count, 1)
    after_own = (stream_own.astype(jnp.float32) + mixed.astype(jnp.float32)).astype(jnp.bfloat16)

    meta = jnp.concatenate(
        [
            route_ids.astype(jnp.float32).T,
            route_weights.T,
            jnp.zeros((8 - 2 * TOP_K, tok_count), jnp.float32),
        ],
        axis=0,
    )
    after_all, meta_all = gather_all(after_own, meta, sp_count, tp_count)

    expert = lax.axis_index("sp").astype(jnp.float32)
    named = (meta_all[:, :TOP_K] == expert).astype(jnp.float32)
    match = jnp.sum(named, axis=1)
    weight = jnp.sum(named * meta_all[:, TOP_K : 2 * TOP_K], axis=1)
    at = jnp.arange(tok_count, dtype=jnp.int32)
    earlier = (at[:, None] < at[None, :]) & (at[:, None] // block_rows == at[None, :] // block_rows)
    before = jnp.dot(
        match.astype(jnp.bfloat16),
        earlier.astype(jnp.bfloat16),
        preferred_element_type=jnp.float32,
    )
    slot_of = before + (at // block_rows * capacity).astype(jnp.float32)[None, :]
    slot_of = jnp.where(match > 0, slot_of, -1.0)
    return experts_all(
        after_all,
        slot_of[:, None],
        weight[:, None],
        ffn_gain[None],
        gate_weight,
        up_weight,
        down_weight,
        after_own,
        capacity,
        sp_count,
        tp_count,
    )


def solution(mesh):
    placed = (
        P("sp", None),
        P(),
        P(None, "tp"),
        P("tp"),
        P(),
        P("sp", None),
        P("sp", None),
        P("sp", None, "tp"),
        P("sp", None, "tp"),
        P("sp", "tp", None),
    )
    square = mesh.shape["tp"] == SIDE * SIDE and mesh.shape["sp"] % CORES == 0
    return jax.shard_map(
        shards if square else shards_any,
        mesh=mesh,
        in_specs=placed,
        out_specs=P("sp", None),
        check_vma=False,
    )
```

```python
import jax
import jax.numpy as jnp
from jax import lax
from jax.experimental import pallas as pl
from jax.experimental.pallas import tpu as pltpu
from jax.sharding import PartitionSpec as P

GROUPS = 4
SPAN = 16
TOP_K = 2
CORES = 2
SIDE = 2
LANES = 128
EPS = 1e-06
MESH = pl.DeviceIdType.MESH
KINDS = 14
X, Y, DX, DY, XP, YP, FX, FY, FDX, FDY, GX, GY, GDX, GDY = range(KINDS)

def from_behind(value, axis, steps):
    count = lax.axis_size(axis)
    first, last = (max(0, -steps), min(count, count - steps))
    return lax.ppermute(value, axis, [(source, source + steps) for source in range(first, last)])


def rms_scale(values, gain):
    return values * lax.rsqrt(jnp.mean(values * values, axis=-1, keepdims=True) + EPS) * gain


def slot_table(chosen_ids, experts, capacity):
    flat_ids = chosen_ids.reshape(-1)
    matches = (flat_ids[:, None] == jnp.arange(experts, dtype=jnp.int32)[None, :]).astype(jnp.int32)
    before = jnp.cumsum(matches, axis=0) - matches
    slot_of = jnp.sum(before * matches, axis=1)
    target = flat_ids * capacity + slot_of
    return (target[:, None] == jnp.arange(experts * capacity, dtype=jnp.int32)[None, :]).astype(
        jnp.float32
    )


def shards_any(
    residual_in,
    mix_gain,
    pool_weight,
    pool_scale,
    ffn_gain,
    route_ids,
    route_weights,
    gate_weight,
    up_weight,
    down_weight,
):
    tp_count = lax.axis_size("tp")
    sp_count = lax.axis_size("sp")
    tp_index = lax.axis_index("tp")
    tok_count, width = residual_in.shape
    group_width = width // GROUPS
    col_count = pool_weight.shape[1]
    row_count = tok_count // tp_count
    capacity = 2 * TOP_K * row_count // sp_count
    group_index = tp_index * col_count // group_width
    window = jnp.power(2, group_index + 1)
    stream = residual_in.astype(jnp.float32)
    inverse = lax.rsqrt(jnp.mean(stream * stream, axis=-1, keepdims=True) + EPS)
    stream_group = lax.dynamic_slice_in_dim(stream, group_index * group_width, group_width, 1)
    gain_group = lax.dynamic_slice_in_dim(mix_gain, group_index * group_width, group_width, 0)
    normed_group = (stream_group * inverse * gain_group).astype(jnp.bfloat16)
    rim_rows = from_behind(normed_group[tok_count - SPAN :], "sp", 1)
    extended = jnp.concatenate([rim_rows, normed_group], axis=0).astype(jnp.float32)
    window_sum = jnp.zeros((tok_count, group_width), jnp.float32)
    for offset in range(SPAN):
        window_sum = window_sum + jnp.where(
            offset < window, extended[SPAN - offset : SPAN - offset + tok_count], 0.0
        )
    position = lax.axis_index("sp") * tok_count + jnp.arange(tok_count, dtype=jnp.int32)
    divisor = jnp.minimum(position + 1, window).astype(jnp.float32)
    pooled = (window_sum / divisor[:, None] - extended[SPAN:]).astype(jnp.bfloat16)
    mixed = (jnp.dot(pooled, pool_weight, preferred_element_type=jnp.float32) * pool_scale).astype(
        jnp.bfloat16
    )
    stream_own = lax.dynamic_slice_in_dim(stream, tp_index * row_count, row_count, 0)
    mixed_own = lax.all_to_all(mixed, "tp", split_axis=0, concat_axis=1, tiled=True)
    after_own = (stream_own + mixed_own.astype(jnp.float32)).astype(jnp.bfloat16)
    normed_own = rms_scale(after_own.astype(jnp.float32), ffn_gain).astype(jnp.bfloat16)
    ids_own = lax.dynamic_slice_in_dim(route_ids, tp_index * row_count, row_count, 0)
    table_own = slot_table(ids_own, sp_count, capacity)
    repeated = jnp.repeat(normed_own, TOP_K, axis=0)
    outgoing = lax.dot_general(
        table_own.astype(jnp.bfloat16),
        repeated,
        (((0,), (0,)), ((), ())),
        preferred_element_type=jnp.float32,
    )
    outgoing = outgoing.astype(jnp.bfloat16).reshape(sp_count, capacity, width)
    arrived = lax.all_to_all(outgoing, "sp", split_axis=0, concat_axis=0, tiled=True)
    piece = lax.all_gather(arrived, "tp", axis=0, tiled=True)
    flat_rows = piece.reshape(-1, width)
    gate_part = jnp.dot(flat_rows, gate_weight[0], preferred_element_type=jnp.float32)
    up_part = jnp.dot(flat_rows, up_weight[0], preferred_element_type=jnp.float32)
    hidden = (jax.nn.silu(gate_part) * up_part).astype(jnp.bfloat16)
    hidden_all = hidden.reshape(piece.shape[0], piece.shape[1], hidden.shape[1])
    hidden_flat = hidden_all.reshape(-1, hidden_all.shape[-1])
    term = jnp.dot(hidden_flat, down_weight[0], preferred_element_type=jnp.float32)
    summed = lax.psum_scatter(
        term.astype(jnp.bfloat16).astype(jnp.float32).astype(jnp.bfloat16),
        "tp",
        scatter_dimension=0,
        tiled=True,
    )
    expert_out = summed.reshape(sp_count, capacity, width)
    returned_rows = lax.all_to_all(expert_out, "sp", split_axis=0, concat_axis=0, tiled=True)
    weights_own = lax.dynamic_slice_in_dim(route_weights, tp_index * row_count, row_count, 0)
    weight_table = jnp.einsum(
        "rk,rkc->rc", weights_own, table_own.reshape(row_count, TOP_K, sp_count * capacity)
    )
    expert_mix = jnp.dot(
        weight_table,
        returned_rows.reshape(-1, width).astype(jnp.float32),
        precision=lax.Precision.HIGHEST,
    )
    out_own = (after_own.astype(jnp.float32) + expert_mix).astype(jnp.bfloat16)
    return lax.all_gather(out_own, "tp", axis=0, tiled=True)


class Place:
    def __init__(self, send_sem, recv_sem):
        self.sp, self.tp = lax.axis_index("sp"), lax.axis_index("tp")
        self.levels = lax.axis_size("sp") // CORES
        self.z, self.c = self.sp // CORES, self.sp % CORES
        y, x = self.tp // SIDE, self.tp % SIDE
        self.tx = y * SIDE + (1 - x)
        self.ty = (1 - y) * SIDE + x
        self.td = (1 - y) * SIDE + (1 - x)
        self.send_sem, self.recv_sem = send_sem, recv_sem
        partner = self.z * CORES + (1 - self.c)
        self.partner = (partner, self.tp)
        along_x, along_y = (self.sp, self.tx), (self.sp, self.ty)
        self.to = {kind: along_x for kind in (X, XP, DX, FX, FDX, GX, GDX)}
        self.to.update({kind: along_y for kind in (Y, YP, DY, FY, FDY, GY, GDY)})

    def copy(self, kind, index, src, dst):
        return pltpu.make_async_remote_copy(
            src_ref=src,
            dst_ref=dst,
            send_sem=self.send_sem.at[kind, index],
            recv_sem=self.recv_sem.at[kind, index],
            device_id=self.to[kind],
            device_id_type=MESH,
        )

    def offsets(self):
        order = [0]
        for distance in range(1, self.levels):
            order += [-distance, distance]
        return order


def greet(place):
    barrier = pltpu.get_barrier_semaphore()

    def hello(target):
        pl.semaphore_signal(barrier, inc=1, device_id=target, device_id_type=MESH)

    count = lax.axis_size("sp")
    hello(place.to[X])
    hello(place.to[Y])
    for step in range(1, count):
        hello((lax.rem(place.sp + step, count), place.tp))
    pl.semaphore_wait(barrier, count + 1)


def level_order(place):
    everywhere = range(place.levels)
    orders = []
    for z in everywhere:
        offsets = [offset for offset in place.offsets() if 0 <= z + offset < place.levels]
        orders.append([z + offset for offset in offsets])
    steps = []
    for index in everywhere:
        level = jnp.int32(orders[0][index])
        for z in everywhere[1:]:
            level = jnp.where(place.z == z, orders[z][index], level)
        steps.append(level)
    return steps


PLAN = [
    ("spread_line", 0), ("relay", 2), ("relay", 1), ("spread_diagonal", 0), ("spread_line", 1),
    ("spread_last", 0), ("pick", 0), ("grow", 0), ("spread_line", 2), ("shrink", 0),
    ("spread_diagonal", 1), ("relay", 3), ("relay_diagonal", 1), ("spread_last", 1), ("first", 0),
    ("pick", 1), ("relay_diagonal", 2), ("grow", 1), ("shrink", 1), ("spread_line", 3),
    ("spread_diagonal", 2), ("first", 1), ("spread_last", 2), ("relay_diagonal", 3), ("pick", 2),
    ("grow", 2), ("shrink", 2), ("spread_diagonal", 3), ("spread_last", 3), ("first", 2),
    ("pick", 3), ("grow", 3), ("shrink", 3), ("second", 2), ("first", 3), ("third", 2),
    ("second", 3), ("third", 3), ("second", 1), ("second", 0), ("third", 1), ("finish", 0),
]


def schedule(levels):
    if levels == 1 + max(step for _, step in PLAN):
        return PLAN
    plan = []
    for turn in range(levels + 3):
        step = turn - 2
        plan += [("relay", turn), ("relay_diagonal", step)]
        plan += [("spread_line", turn), ("spread_diagonal", turn - 1), ("spread_last", step)]
        plan += [("pick", step), ("first", step - 1), ("grow", step), ("second", step - 2)]
        plan += [("shrink", step), ("third", step - 3)]
    plan += [("second", levels - 1), ("third", levels - 2), ("third", levels - 1), ("finish", 0)]
    return [(stage, step) for stage, step in plan if 0 <= step < levels]


def layer_kernel(
    own_ref, meta_ref, gain_ref, gate_ref, up_ref, down_ref, out_ref,
    held, metas, slot_rows, weight_rows, gu, dn, picked, hid, spread, scale, parts,
    r_pair, s_diag, r_ydiag, r_xdiag, s_x, s_y, r_x, r_y, s_z, r_z,
    send_sem, recv_sem, g_send, g_recv, p_send, p_recv, z_send, z_recv, m_send, m_recv,
    w_sem, l_sem,
):
    place = Place(send_sem, recv_sem)
    rows, cols = own_ref.shape
    width = held.shape[2]
    slots = spread.shape[2]
    sp_count, tiles = lax.axis_size("sp"), SIDE * SIDE
    half = rows // 2
    z, c, tp = place.z, place.c, place.tp
    chunk, wide = 32, 256
    pieces, _, pair_lanes = gu.shape
    lanes_each = pair_lanes // 2
    order = level_order(place)

    def gate_copy(piece, side):
        source = (gate_ref, up_ref)[side]
        return pltpu.make_async_copy(
            source.at[0, :, pl.ds(piece * lanes_each, lanes_each)],
            gu.at[piece, :, pl.ds(side * lanes_each, lanes_each)],
            w_sem.at[piece, side],
        )

    down_copy = pltpu.make_async_copy(down_ref.at[0], dn, w_sem.at[pieces, 0])

    def block(level, core, tile, first=0, count=rows):
        at = pl.ds(pl.multiple_of(core * rows + first, half), count)
        return held.at[level, at, pl.ds(pl.multiple_of(tile * cols, cols), cols)]

    def meta_copy(step):
        return pltpu.make_async_remote_copy(
            src_ref=meta_ref,
            dst_ref=metas.at[place.sp],
            send_sem=m_send.at[step],
            recv_sem=m_recv.at[step],
            device_id=(lax.rem(place.sp + step, sp_count), tp),
            device_id_type=MESH,
        )

    middle = (z > 0) & (z < place.levels - 1)
    has_up, has_down = z < place.levels - 1, z > 0

    def line(level, diagonal, up=True):
        ref = block(level, c, place.td if diagonal else tp)
        return pltpu.make_async_remote_copy(
            src_ref=ref,
            dst_ref=ref,
            send_sem=z_send.at[2 * diagonal + up, level],
            recv_sem=z_recv.at[diagonal, level],
            device_id=((z + 1 if up else z - 1) * CORES + c, tp),
            device_id_type=MESH,
        )

    def line_own(diagonal, act):
        pl.when(has_up)(lambda: act(line(z, diagonal, True)))
        pl.when(has_down)(lambda: act(line(z, diagonal, False)))

    def line_on(level, diagonal, act):
        pl.when(middle & (level < z))(lambda: act(line(level, diagonal, True)))
        pl.when(middle & (level > z))(lambda: act(line(level, diagonal, False)))

    def line_relay(step, diagonal):
        level = order[step]
        if step:
            pl.when(middle)(lambda: line(level, diagonal).wait_recv())
            line_on(level, diagonal, lambda copy: copy.start())

    def line_end(level, diagonal):
        pl.when(jnp.logical_not(middle))(lambda: line(level, diagonal).wait_recv())

    def core_copy(level, tile, core):
        ref = block(level, core, tile)
        return pltpu.make_async_remote_copy(
            src_ref=ref,
            dst_ref=ref,
            send_sem=g_send.at[level, tile],
            recv_sem=g_recv.at[level, tile],
            device_id=place.partner,
            device_id_type=MESH,
        )

    def whole(kind, level, tile):
        ref = block(level, c, tile)
        return place.copy(kind, level, ref, ref)

    def part(kind, level, tile):
        ref = block(level, c, tile, 0 if kind == GDY else half, half)
        return place.copy(kind, level, ref, ref)

    def spread_line(step):
        level = order[step]
        if step:
            line_end(level, 0)
        whole(GX, level, tp).start()
        whole(GY, level, tp).start()
        core_copy(level, tp, c).start()

    def spread_diagonal(step):
        level = order[step]
        whole(GX, level, place.tx).wait_recv()
        if step == 0:
            part(GDY, level, place.tx).start()
        core_copy(level, place.tx, c).start()
        whole(GY, level, place.ty).wait_recv()
        if step == 0:
            part(GDX, level, place.ty).start()
        core_copy(level, place.ty, c).start()

    def spread_last(step):
        level = order[step]
        if step:
            line_end(level, 1)
        else:
            part(GDY, level, place.td).wait_recv()
            part(GDX, level, place.td).wait_recv()
            line_own(1, lambda copy: copy.start())
        core_copy(level, place.td, c).start()

    def number_slots():
        for hop in range(1, sp_count):
            meta_copy(hop).wait_recv()
        expert = place.sp.astype(jnp.float32)
        match = jnp.zeros((sp_count, rows), jnp.float32)
        weight = jnp.zeros((sp_count, rows), jnp.float32)
        for k in range(TOP_K):
            named = jnp.where(metas[:, k] == expert, 1.0, 0.0)
            match = match + named
            weight = weight + named * metas[:, TOP_K + k]
        block_rows = rows // tiles
        source = lax.broadcasted_iota(jnp.int32, (rows, rows), 0)
        target = lax.broadcasted_iota(jnp.int32, (rows, rows), 1)
        earlier = (source < target) & (source // block_rows == target // block_rows)
        earlier = jnp.where(earlier, 1.0, 0.0).astype(jnp.bfloat16)
        before = jnp.dot(match.astype(jnp.bfloat16), earlier, preferred_element_type=jnp.float32)
        at = lax.broadcasted_iota(jnp.int32, (sp_count, rows), 1)
        base = (at // block_rows * (slots // tiles)).astype(jnp.float32)
        slot_rows[...] = jnp.where(match > 0, before + base, -1.0)
        weight_rows[...] = weight

    def pick(step):
        level = order[step]
        if step == 0:
            number_slots()
        for tile in range(tiles):
            core_copy(level, tile, 1 - c).wait_recv()
        for b in range(CORES):
            source = pl.ds(level * CORES + b, 1)
            at = lax.broadcasted_iota(jnp.int32, (slots, rows), 0).astype(jnp.float32)
            chosen = at == slot_rows[source]
            table = jnp.where(chosen, 1.0, 0.0)
            scale[b] = jnp.sum(jnp.where(chosen, weight_rows[source], 0.0), axis=1, keepdims=True)
            spread[b] = table.T.astype(jnp.bfloat16)
            table = table.astype(jnp.bfloat16)
            squares = jnp.zeros((slots, 1), jnp.float32)
            into = slice(b * slots, (b + 1) * slots)
            for start in range(0, width, wide):
                lanes = slice(start, start + wide)
                value = jnp.dot(
                    table,
                    held[level, b * rows : (b + 1) * rows, lanes],
                    preferred_element_type=jnp.float32,
                )
                squares = squares + jnp.sum(value * value, axis=1, keepdims=True)
                picked[into, lanes] = value.astype(jnp.bfloat16)
            inverse = lax.rsqrt(squares / width + EPS)
            for start in range(0, width, wide):
                lanes = slice(start, start + wide)
                value = picked[into, lanes].astype(jnp.float32) * inverse * gain_ref[:, lanes]
                picked[into, lanes] = value.astype(jnp.bfloat16)

    def grow(step):
        for piece in range(pieces):
            if step == 0:
                gate_copy(piece, 0).wait()
                gate_copy(piece, 1).wait()
            both = jnp.dot(picked[...], gu[piece], preferred_element_type=jnp.float32)
            gate, up = both[:, :lanes_each], both[:, lanes_each:]
            lanes = slice(piece * lanes_each, (piece + 1) * lanes_each)
            hid[:, lanes] = (jax.nn.silu(gate) * up).astype(jnp.bfloat16)

    def pair_copy(level, tile):
        lanes = pl.ds(pl.multiple_of(tile * cols, cols), cols)
        return pltpu.make_async_remote_copy(
            src_ref=parts.at[level, 1 - c, :, lanes],
            dst_ref=r_pair.at[level, :, lanes],
            send_sem=p_send.at[level, tile],
            recv_sem=p_recv.at[level, tile],
            device_id=place.partner,
            device_id_type=MESH,
        )

    def shrink(step):
        level = order[step]
        if step == 0:
            down_copy.wait()
        for tile in (place.td, place.tx, place.ty, tp):
            lanes = pl.ds(pl.multiple_of(tile * cols, cols), cols)
            term = jnp.dot(hid[...], dn[:, lanes], preferred_element_type=jnp.float32)
            for b in range(CORES):
                scaled = (term[b * slots : (b + 1) * slots] * scale[b]).astype(jnp.bfloat16)
                value = jnp.dot(spread[b], scaled, preferred_element_type=jnp.float32)
                parts[level, b, :, lanes] = value.astype(jnp.bfloat16)
            pair_copy(level, tile).start()

    def summed(level, tile, row, count=chunk):
        at = pl.ds(pl.multiple_of(row, chunk), count)
        lanes = pl.ds(pl.multiple_of(tile * cols, cols), cols)
        mine = parts[level, c, at, lanes].astype(jnp.float32)
        return mine + r_pair[level, at, lanes].astype(jnp.float32)

    def over(first, last, body):
        def step(index, carry):
            body(pl.multiple_of(first + index * chunk, chunk))
            return carry

        lax.fori_loop(0, (last - first) // chunk, step, 0)

    def diag(kind, level):
        if kind == DY:
            return place.copy(kind, level, s_diag.at[level, pl.ds(0, half)], r_ydiag.at[level])
        return place.copy(kind, level, s_diag.at[level, pl.ds(half, half)], r_xdiag.at[level])

    def side(kind, level):
        source, arrived = (s_x, r_x) if kind in (X, XP) else (s_y, r_y)
        at = pl.ds(0 if kind in (X, YP) else half, half)
        return place.copy(kind, level, source.at[level, at], arrived.at[level, at])

    def owner_copy(level, part_of, arriving):
        at = pl.ds(part_of * half, half)
        return pltpu.make_async_remote_copy(
            src_ref=s_z.at[level, at],
            dst_ref=r_z.at[level if arriving else z, at],
            send_sem=z_send.at[4 + part_of, level],
            recv_sem=z_recv.at[2 + part_of, level if arriving else z],
            device_id=(level * CORES + c, tp),
            device_id_type=MESH,
        )

    def first(step):
        level = order[step]

        def plain(buffer, tile):
            def body(row):
                buffer[level, pl.ds(row, chunk)] = summed(level, tile, row).astype(jnp.bfloat16)

            return body

        pair_copy(level, place.td).wait_recv()
        over(0, half, plain(s_diag, place.td))
        diag(DY, level).start()
        over(half, rows, plain(s_diag, place.td))
        diag(DX, level).start()
        pair_copy(level, place.tx).wait_recv()
        over(half, rows, plain(s_x, place.tx))
        side(XP, level).start()
        pair_copy(level, place.ty).wait_recv()
        over(0, half, plain(s_y, place.ty))
        side(YP, level).start()

    def second(step):
        level = order[step]

        def joined(buffer, tile, arrived, base):
            def body(row):
                other = arrived[level, pl.ds(pl.multiple_of(row - base, chunk), chunk)]
                total = summed(level, tile, row) + other.astype(jnp.float32)
                buffer[level, pl.ds(row, chunk)] = total.astype(jnp.bfloat16)

            return body

        diag(DY, level).wait_recv()
        over(0, half, joined(s_x, place.tx, r_ydiag, 0))
        side(X, level).start()
        diag(DX, level).wait_recv()
        over(half, rows, joined(s_y, place.ty, r_xdiag, half))
        side(Y, level).start()

    def plane_sum(level, row):
        at = pl.ds(row, chunk)
        total = summed(level, tp, row)
        return total + r_x[level, at].astype(jnp.float32) + r_y[level, at].astype(jnp.float32)

    def plane_wait(level, part_of):
        if part_of == 0:
            pair_copy(level, tp).wait_recv()
        for kind in ((X, YP), (XP, Y))[part_of]:
            side(kind, level).wait_recv()

    def third(step):
        if step == 0:
            return
        level = order[step]

        def body(row):
            s_z[level, pl.ds(row, chunk)] = plane_sum(level, row).astype(jnp.bfloat16)

        for part_of in range(2):
            plane_wait(level, part_of)
            over(part_of * half, (part_of + 1) * half, body)
            owner_copy(level, part_of, False).start()

    def final(kind, tile, part_of):
        at = pl.ds(part_of * half, half)
        ref = out_ref.at[at, pl.ds(pl.multiple_of(tile * cols, cols), cols)]
        return place.copy(kind, part_of, ref, ref)

    def finish(step):
        level = order[step]

        def body(row):
            at = pl.ds(row, chunk)
            total = plane_sum(level, row)
            for other in order[1:]:
                total = total + r_z[other, at].astype(jnp.float32)
            total = total + own_ref[at].astype(jnp.float32)
            lanes = pl.ds(pl.multiple_of(tp * cols, cols), cols)
            out_ref[at, lanes] = total.astype(jnp.bfloat16)

        for part_of in range(2):
            plane_wait(level, part_of)
            for other in order[1:]:
                owner_copy(other, part_of, True).wait_recv()
            over(part_of * half, (part_of + 1) * half, body)
            final(FX, tp, part_of).start()
            final(FY, tp, part_of).start()

    local = pltpu.make_async_copy(own_ref, block(z, c, tp), l_sem.at[0])
    local.start()
    local_meta = pltpu.make_async_copy(meta_ref, metas.at[place.sp], l_sem.at[1])
    local_meta.start()
    for piece in range(pieces):
        gate_copy(piece, 0).start()
        gate_copy(piece, 1).start()
    down_copy.start()
    local.wait()
    local_meta.wait()
    greet(place)
    for hop in range(1, sp_count):
        meta_copy(hop).start()
    line_own(0, lambda copy: copy.start())

    stages = {
        "relay": lambda step: line_relay(step, 0),
        "relay_diagonal": lambda step: line_relay(step, 1),
        "spread_line": spread_line,
        "spread_diagonal": spread_diagonal,
        "spread_last": spread_last,
        "pick": pick,
        "grow": grow,
        "shrink": shrink,
        "first": first,
        "second": second,
        "third": third,
        "finish": finish,
    }
    for stage, step in schedule(place.levels):
        stages[stage](step)

    final(FX, place.tx, 0).wait_recv()
    final(FDY, place.tx, 0).start()
    final(FY, place.ty, 0).wait_recv()
    final(FY, place.ty, 1).wait_recv()
    final(FDX, place.ty, 1).start()
    final(FX, place.tx, 1).wait_recv()
    for hop in range(1, sp_count):
        meta_copy(hop).wait_send()
    line_own(0, lambda copy: copy.wait_send())
    line_own(1, lambda copy: copy.wait_send())
    for step, level in enumerate(order):
        whole(GX, level, tp).wait_send()
        whole(GY, level, tp).wait_send()
        for tile in range(tiles):
            core_copy(level, tile, c).wait_send()
            pair_copy(level, tile).wait_send()
        for kind in (DX, DY):
            diag(kind, level).wait_send()
        for kind in (X, Y, XP, YP):
            side(kind, level).wait_send()
        if step:
            for part_of in range(2):
                line_on(level, part_of, lambda copy: copy.wait_send())
                owner_copy(level, part_of, False).wait_send()
        else:
            part(GDY, level, place.tx).wait_send()
            part(GDX, level, place.ty).wait_send()
    final(FDY, place.td, 0).wait_recv()
    final(FDX, place.td, 1).wait_recv()
    for part_of in range(2):
        final(FX, tp, part_of).wait_send()
        final(FY, tp, part_of).wait_send()
    final(FDY, place.tx, 0).wait_send()
    final(FDX, place.ty, 1).wait_send()


def layer_all(own, meta, gain, gate, up, down, capacity, sp_count, tp_count):
    rows, cols = own.shape
    width = tp_count * cols
    hidden = gate.shape[2]
    levels = sp_count // CORES
    slots = capacity * tp_count
    vmem = pl.BlockSpec(memory_space=pltpu.VMEM)
    hbm = pl.BlockSpec(memory_space=pl.ANY)
    whole = pltpu.VMEM((levels, rows, cols), jnp.bfloat16)
    halved = pltpu.VMEM((levels, rows // 2, cols), jnp.bfloat16)
    pieces = hidden // LANES
    return pl.pallas_call(
        layer_kernel,
        out_shape=jax.ShapeDtypeStruct((rows, width), own.dtype),
        in_specs=[vmem, vmem, vmem, hbm, hbm, hbm],
        out_specs=vmem,
        scratch_shapes=[
            pltpu.VMEM((levels, CORES * rows, width), jnp.bfloat16),
            pltpu.VMEM((sp_count,) + meta.shape, jnp.float32),
            pltpu.VMEM((sp_count, rows), jnp.float32),
            pltpu.VMEM((sp_count, rows), jnp.float32),
            pltpu.VMEM((pieces, width, 2 * LANES), jnp.bfloat16),
            pltpu.VMEM((hidden, width), jnp.bfloat16),
            pltpu.VMEM((CORES * slots, width), jnp.bfloat16),
            pltpu.VMEM((CORES * slots, hidden), jnp.bfloat16),
            pltpu.VMEM((CORES, rows, slots), jnp.bfloat16),
            pltpu.VMEM((CORES, slots, 1), jnp.float32),
            pltpu.VMEM((levels, CORES, rows, width), jnp.bfloat16),
            pltpu.VMEM((levels, rows, width), jnp.bfloat16),
            whole, halved, halved, whole, whole, whole, whole, whole, whole,
            pltpu.SemaphoreType.DMA((KINDS, max(2, levels))),
            pltpu.SemaphoreType.DMA((KINDS, max(2, levels))),
            pltpu.SemaphoreType.DMA((levels, tp_count)),
            pltpu.SemaphoreType.DMA((levels, tp_count)),
            pltpu.SemaphoreType.DMA((levels, tp_count)),
            pltpu.SemaphoreType.DMA((levels, tp_count)),
            pltpu.SemaphoreType.DMA((6, levels)),
            pltpu.SemaphoreType.DMA((4, levels)),
            pltpu.SemaphoreType.DMA((sp_count,)),
            pltpu.SemaphoreType.DMA((sp_count,)),
            pltpu.SemaphoreType.DMA((pieces + 1, 2)),
            pltpu.SemaphoreType.DMA((2,)),
        ],
        compiler_params=pltpu.CompilerParams(
            collective_id=0, has_side_effects=True, vmem_limit_bytes=62 * 1024 * 1024
        ),
        name="layer_all",
    )(own, meta, gain, gate, up, down)


def shards(
    residual_in,
    mix_gain,
    pool_weight,
    pool_scale,
    ffn_gain,
    route_ids,
    route_weights,
    gate_weight,
    up_weight,
    down_weight,
):
    tp_count = lax.axis_size("tp")
    sp_count = lax.axis_size("sp")
    tp_index = lax.axis_index("tp")
    tok_count, width = residual_in.shape
    group_width = width // GROUPS
    col_count = pool_weight.shape[1]
    block_rows = tok_count // tp_count
    capacity = 2 * TOP_K * block_rows // sp_count
    group_index = tp_index * col_count // group_width
    window = jnp.power(2, group_index + 1)
    stream = residual_in.astype(jnp.float32)
    inverse = lax.rsqrt(jnp.mean(stream * stream, axis=-1, keepdims=True) + EPS)
    stream_group = lax.dynamic_slice_in_dim(residual_in, group_index * group_width, group_width, 1)
    stream_group = stream_group.astype(jnp.float32)
    gain_group = lax.dynamic_slice_in_dim(mix_gain, group_index * group_width, group_width, 0)
    normed_group = (stream_group * inverse * gain_group).astype(jnp.bfloat16)
    rim_rows = from_behind(normed_group[tok_count - SPAN :], "sp", 1)
    extended = jnp.concatenate([rim_rows, normed_group], axis=0).astype(jnp.float32)
    window_sum = jnp.zeros((tok_count, group_width), jnp.float32)
    for offset in range(SPAN):
        window_sum = window_sum + jnp.where(
            offset < window, extended[SPAN - offset : SPAN - offset + tok_count], 0.0
        )
    position = lax.axis_index("sp") * tok_count + jnp.arange(tok_count, dtype=jnp.int32)
    divisor = jnp.minimum(position + 1, window).astype(jnp.float32)
    pooled = (window_sum / divisor[:, None] - extended[SPAN:]).astype(jnp.bfloat16)
    mixed = (jnp.dot(pooled, pool_weight, preferred_element_type=jnp.float32) * pool_scale).astype(
        jnp.bfloat16
    )
    stream_own = lax.dynamic_slice_in_dim(residual_in, tp_index * col_count, col_count, 1)
    after_own = (stream_own.astype(jnp.float32) + mixed.astype(jnp.float32)).astype(jnp.bfloat16)

    meta = jnp.concatenate(
        [
            route_ids.astype(jnp.float32).T,
            route_weights.T,
            jnp.zeros((8 - 2 * TOP_K, tok_count), jnp.float32),
        ],
        axis=0,
    )
    return layer_all(
        after_own,
        meta,
        ffn_gain[None],
        gate_weight,
        up_weight,
        down_weight,
        capacity,
        sp_count,
        tp_count,
    )


def solution(mesh):
    placed = (
        P("sp", None),
        P(),
        P(None, "tp"),
        P("tp"),
        P(),
        P("sp", None),
        P("sp", None),
        P("sp", None, "tp"),
        P("sp", None, "tp"),
        P("sp", "tp", None),
    )
    square = mesh.shape["tp"] == SIDE * SIDE and mesh.shape["sp"] % CORES == 0
    return jax.shard_map(
        shards if square else shards_any,
        mesh=mesh,
        in_specs=placed,
        out_specs=P("sp", None),
        check_vma=False,
    )
```

```python
import jax
import jax.numpy as jnp
from jax import lax
from jax.experimental import pallas as pl
from jax.experimental.pallas import tpu as pltpu
from jax.sharding import PartitionSpec as P

GROUPS = 4
SPAN = 16
TOP_K = 2
CORES = 2
SIDE = 2
LANES = 128
EPS = 1e-06
MESH = pl.DeviceIdType.MESH
KINDS = 14
X, Y, DX, DY, XP, YP, FX, FY, FDX, FDY, GX, GY, GDX, GDY = range(KINDS)

def from_behind(value, axis, steps):
    count = lax.axis_size(axis)
    first, last = (max(0, -steps), min(count, count - steps))
    return lax.ppermute(value, axis, [(source, source + steps) for source in range(first, last)])


def rms_scale(values, gain):
    return values * lax.rsqrt(jnp.mean(values * values, axis=-1, keepdims=True) + EPS) * gain


def slot_table(chosen_ids, experts, capacity):
    flat_ids = chosen_ids.reshape(-1)
    matches = (flat_ids[:, None] == jnp.arange(experts, dtype=jnp.int32)[None, :]).astype(jnp.int32)
    before = jnp.cumsum(matches, axis=0) - matches
    slot_of = jnp.sum(before * matches, axis=1)
    target = flat_ids * capacity + slot_of
    return (target[:, None] == jnp.arange(experts * capacity, dtype=jnp.int32)[None, :]).astype(
        jnp.float32
    )


def shards_any(
    residual_in,
    mix_gain,
    pool_weight,
    pool_scale,
    ffn_gain,
    route_ids,
    route_weights,
    gate_weight,
    up_weight,
    down_weight,
):
    tp_count = lax.axis_size("tp")
    sp_count = lax.axis_size("sp")
    tp_index = lax.axis_index("tp")
    tok_count, width = residual_in.shape
    group_width = width // GROUPS
    col_count = pool_weight.shape[1]
    row_count = tok_count // tp_count
    capacity = 2 * TOP_K * row_count // sp_count
    group_index = tp_index * col_count // group_width
    window = jnp.power(2, group_index + 1)
    stream = residual_in.astype(jnp.float32)
    inverse = lax.rsqrt(jnp.mean(stream * stream, axis=-1, keepdims=True) + EPS)
    stream_group = lax.dynamic_slice_in_dim(stream, group_index * group_width, group_width, 1)
    gain_group = lax.dynamic_slice_in_dim(mix_gain, group_index * group_width, group_width, 0)
    normed_group = (stream_group * inverse * gain_group).astype(jnp.bfloat16)
    rim_rows = from_behind(normed_group[tok_count - SPAN :], "sp", 1)
    extended = jnp.concatenate([rim_rows, normed_group], axis=0).astype(jnp.float32)
    window_sum = jnp.zeros((tok_count, group_width), jnp.float32)
    for offset in range(SPAN):
        window_sum = window_sum + jnp.where(
            offset < window, extended[SPAN - offset : SPAN - offset + tok_count], 0.0
        )
    position = lax.axis_index("sp") * tok_count + jnp.arange(tok_count, dtype=jnp.int32)
    divisor = jnp.minimum(position + 1, window).astype(jnp.float32)
    pooled = (window_sum / divisor[:, None] - extended[SPAN:]).astype(jnp.bfloat16)
    mixed = (jnp.dot(pooled, pool_weight, preferred_element_type=jnp.float32) * pool_scale).astype(
        jnp.bfloat16
    )
    stream_own = lax.dynamic_slice_in_dim(stream, tp_index * row_count, row_count, 0)
    mixed_own = lax.all_to_all(mixed, "tp", split_axis=0, concat_axis=1, tiled=True)
    after_own = (stream_own + mixed_own.astype(jnp.float32)).astype(jnp.bfloat16)
    normed_own = rms_scale(after_own.astype(jnp.float32), ffn_gain).astype(jnp.bfloat16)
    ids_own = lax.dynamic_slice_in_dim(route_ids, tp_index * row_count, row_count, 0)
    table_own = slot_table(ids_own, sp_count, capacity)
    repeated = jnp.repeat(normed_own, TOP_K, axis=0)
    outgoing = lax.dot_general(
        table_own.astype(jnp.bfloat16),
        repeated,
        (((0,), (0,)), ((), ())),
        preferred_element_type=jnp.float32,
    )
    outgoing = outgoing.astype(jnp.bfloat16).reshape(sp_count, capacity, width)
    arrived = lax.all_to_all(outgoing, "sp", split_axis=0, concat_axis=0, tiled=True)
    piece = lax.all_gather(arrived, "tp", axis=0, tiled=True)
    flat_rows = piece.reshape(-1, width)
    gate_part = jnp.dot(flat_rows, gate_weight[0], preferred_element_type=jnp.float32)
    up_part = jnp.dot(flat_rows, up_weight[0], preferred_element_type=jnp.float32)
    hidden = (jax.nn.silu(gate_part) * up_part).astype(jnp.bfloat16)
    hidden_all = hidden.reshape(piece.shape[0], piece.shape[1], hidden.shape[1])
    hidden_flat = hidden_all.reshape(-1, hidden_all.shape[-1])
    term = jnp.dot(hidden_flat, down_weight[0], preferred_element_type=jnp.float32)
    summed = lax.psum_scatter(
        term.astype(jnp.bfloat16).astype(jnp.float32).astype(jnp.bfloat16),
        "tp",
        scatter_dimension=0,
        tiled=True,
    )
    expert_out = summed.reshape(sp_count, capacity, width)
    returned_rows = lax.all_to_all(expert_out, "sp", split_axis=0, concat_axis=0, tiled=True)
    weights_own = lax.dynamic_slice_in_dim(route_weights, tp_index * row_count, row_count, 0)
    weight_table = jnp.einsum(
        "rk,rkc->rc", weights_own, table_own.reshape(row_count, TOP_K, sp_count * capacity)
    )
    expert_mix = jnp.dot(
        weight_table,
        returned_rows.reshape(-1, width).astype(jnp.float32),
        precision=lax.Precision.HIGHEST,
    )
    out_own = (after_own.astype(jnp.float32) + expert_mix).astype(jnp.bfloat16)
    return lax.all_gather(out_own, "tp", axis=0, tiled=True)


class Place:
    def __init__(self, send_sem, recv_sem):
        self.sp, self.tp = lax.axis_index("sp"), lax.axis_index("tp")
        self.levels = lax.axis_size("sp") // CORES
        self.z, self.c = self.sp // CORES, self.sp % CORES
        y, x = self.tp // SIDE, self.tp % SIDE
        self.tx = y * SIDE + (1 - x)
        self.ty = (1 - y) * SIDE + x
        self.td = (1 - y) * SIDE + (1 - x)
        self.send_sem, self.recv_sem = send_sem, recv_sem
        partner = self.z * CORES + (1 - self.c)
        self.partner = (partner, self.tp)
        along_x, along_y = (self.sp, self.tx), (self.sp, self.ty)
        self.to = {kind: along_x for kind in (X, XP, DX, FX, FDX, GX, GDX)}
        self.to.update({kind: along_y for kind in (Y, YP, DY, FY, FDY, GY, GDY)})

    def copy(self, kind, index, src, dst):
        return pltpu.make_async_remote_copy(
            src_ref=src,
            dst_ref=dst,
            send_sem=self.send_sem.at[kind, index],
            recv_sem=self.recv_sem.at[kind, index],
            device_id=self.to[kind],
            device_id_type=MESH,
        )

    def offsets(self):
        order = [0]
        for distance in range(1, self.levels):
            order += [-distance, distance]
        return order


def greet(place):
    barrier = pltpu.get_barrier_semaphore()

    def hello(target):
        pl.semaphore_signal(barrier, inc=1, device_id=target, device_id_type=MESH)

    count = lax.axis_size("sp")
    hello(place.to[X])
    hello(place.to[Y])
    for step in range(1, count):
        hello((lax.rem(place.sp + step, count), place.tp))
    pl.semaphore_wait(barrier, count + 1)


def level_order(place):
    everywhere = range(place.levels)
    orders = []
    for z in everywhere:
        offsets = [offset for offset in place.offsets() if 0 <= z + offset < place.levels]
        orders.append([z + offset for offset in offsets])
    steps = []
    for index in everywhere:
        level = jnp.int32(orders[0][index])
        for z in everywhere[1:]:
            level = jnp.where(place.z == z, orders[z][index], level)
        steps.append(level)
    return steps


PLAN = [
    ("spread_line", 0), ("relay", 2), ("relay", 1), ("spread_diagonal", 0), ("spread_line", 1),
    ("spread_last", 0), ("pick", 0), ("grow", 0), ("spread_line", 2), ("shrink", 0),
    ("spread_diagonal", 1), ("relay", 3), ("relay_diagonal", 1), ("spread_last", 1), ("first", 0),
    ("pick", 1), ("relay_diagonal", 2), ("grow", 1), ("shrink", 1), ("spread_line", 3),
    ("spread_diagonal", 2), ("first", 1), ("spread_last", 2), ("relay_diagonal", 3), ("pick", 2),
    ("grow", 2), ("shrink", 2), ("spread_diagonal", 3), ("spread_last", 3), ("first", 2),
    ("pick", 3), ("grow", 3), ("shrink", 3), ("second", 2), ("first", 3), ("third", 2),
    ("second", 3), ("third", 3), ("second", 1), ("second", 0), ("third", 1), ("finish", 0),
]


def schedule(levels):
    if levels == 1 + max(step for _, step in PLAN):
        return PLAN
    plan = []
    for turn in range(levels + 3):
        step = turn - 2
        plan += [("relay", turn), ("relay_diagonal", step)]
        plan += [("spread_line", turn), ("spread_diagonal", turn - 1), ("spread_last", step)]
        plan += [("pick", step), ("first", step - 1), ("grow", step), ("second", step - 2)]
        plan += [("shrink", step), ("third", step - 3)]
    plan += [("second", levels - 1), ("third", levels - 2), ("third", levels - 1), ("finish", 0)]
    return [(stage, step) for stage, step in plan if 0 <= step < levels]


def layer_kernel(
    stream_ref, mix_ref, pool_ref, pool_scale_ref, ids_ref, shares_ref,
    gain_ref, gate_ref, up_ref, down_ref, out_ref,
    own_ref, extended, rim_out, rim_in, meta_ref, held, metas, slot_rows, weight_rows, gu, dn, picked, hid, spread, scale, parts,
    r_pair, s_diag, r_ydiag, r_xdiag, s_x, s_y, r_x, r_y, s_z, r_z,
    send_sem, recv_sem, g_send, g_recv, p_send, p_recv, z_send, z_recv, m_send, m_recv,
    w_sem, l_sem, rim_send, rim_recv,
):
    place = Place(send_sem, recv_sem)
    rows, cols = own_ref.shape
    width = held.shape[2]
    slots = spread.shape[2]
    sp_count, tiles = lax.axis_size("sp"), SIDE * SIDE
    half = rows // 2
    z, c, tp = place.z, place.c, place.tp
    chunk, wide = 32, 256
    pieces, _, pair_lanes = gu.shape
    lanes_each = pair_lanes // 2
    order = level_order(place)

    def gate_copy(piece, side):
        source = (gate_ref, up_ref)[side]
        return pltpu.make_async_copy(
            source.at[0, :, pl.ds(piece * lanes_each, lanes_each)],
            gu.at[piece, :, pl.ds(side * lanes_each, lanes_each)],
            w_sem.at[piece, side],
        )

    down_copy = pltpu.make_async_copy(down_ref.at[0], dn, w_sem.at[pieces, 0])

    def block(level, core, tile, first=0, count=rows):
        at = pl.ds(pl.multiple_of(core * rows + first, half), count)
        return held.at[level, at, pl.ds(pl.multiple_of(tile * cols, cols), cols)]

    def meta_copy(step):
        return pltpu.make_async_remote_copy(
            src_ref=meta_ref,
            dst_ref=metas.at[place.sp],
            send_sem=m_send.at[step],
            recv_sem=m_recv.at[step],
            device_id=(lax.rem(place.sp + step, sp_count), tp),
            device_id_type=MESH,
        )

    middle = (z > 0) & (z < place.levels - 1)
    has_up, has_down = z < place.levels - 1, z > 0

    def line(level, diagonal, up=True):
        ref = block(level, c, place.td if diagonal else tp)
        return pltpu.make_async_remote_copy(
            src_ref=ref,
            dst_ref=ref,
            send_sem=z_send.at[2 * diagonal + up, level],
            recv_sem=z_recv.at[diagonal, level],
            device_id=((z + 1 if up else z - 1) * CORES + c, tp),
            device_id_type=MESH,
        )

    def line_own(diagonal, act):
        pl.when(has_up)(lambda: act(line(z, diagonal, True)))
        pl.when(has_down)(lambda: act(line(z, diagonal, False)))

    def line_on(level, diagonal, act):
        pl.when(middle & (level < z))(lambda: act(line(level, diagonal, True)))
        pl.when(middle & (level > z))(lambda: act(line(level, diagonal, False)))

    def line_relay(step, diagonal):
        level = order[step]
        if step:
            pl.when(middle)(lambda: line(level, diagonal).wait_recv())
            line_on(level, diagonal, lambda copy: copy.start())

    def line_end(level, diagonal):
        pl.when(jnp.logical_not(middle))(lambda: line(level, diagonal).wait_recv())

    def core_copy(level, tile, core):
        ref = block(level, core, tile)
        return pltpu.make_async_remote_copy(
            src_ref=ref,
            dst_ref=ref,
            send_sem=g_send.at[level, tile],
            recv_sem=g_recv.at[level, tile],
            device_id=place.partner,
            device_id_type=MESH,
        )

    def whole(kind, level, tile):
        ref = block(level, c, tile)
        return place.copy(kind, level, ref, ref)

    def part(kind, level, tile):
        ref = block(level, c, tile, 0 if kind == GDY else half, half)
        return place.copy(kind, level, ref, ref)

    def spread_line(step):
        level = order[step]
        if step:
            line_end(level, 0)
        whole(GX, level, tp).start()
        whole(GY, level, tp).start()
        core_copy(level, tp, c).start()

    def spread_diagonal(step):
        level = order[step]
        whole(GX, level, place.tx).wait_recv()
        if step == 0:
            part(GDY, level, place.tx).start()
        core_copy(level, place.tx, c).start()
        whole(GY, level, place.ty).wait_recv()
        if step == 0:
            part(GDX, level, place.ty).start()
        core_copy(level, place.ty, c).start()

    def spread_last(step):
        level = order[step]
        if step:
            line_end(level, 1)
        else:
            part(GDY, level, place.td).wait_recv()
            part(GDX, level, place.td).wait_recv()
            line_own(1, lambda copy: copy.start())
        core_copy(level, place.td, c).start()

    def number_slots():
        for hop in range(1, sp_count):
            meta_copy(hop).wait_recv()
        expert = place.sp.astype(jnp.float32)
        match = jnp.zeros((sp_count, rows), jnp.float32)
        weight = jnp.zeros((sp_count, rows), jnp.float32)
        for k in range(TOP_K):
            named = jnp.where(metas[:, k] == expert, 1.0, 0.0)
            match = match + named
            weight = weight + named * metas[:, TOP_K + k]
        block_rows = rows // tiles
        source = lax.broadcasted_iota(jnp.int32, (rows, rows), 0)
        target = lax.broadcasted_iota(jnp.int32, (rows, rows), 1)
        earlier = (source < target) & (source // block_rows == target // block_rows)
        earlier = jnp.where(earlier, 1.0, 0.0).astype(jnp.bfloat16)
        before = jnp.dot(match.astype(jnp.bfloat16), earlier, preferred_element_type=jnp.float32)
        at = lax.broadcasted_iota(jnp.int32, (sp_count, rows), 1)
        base = (at // block_rows * (slots // tiles)).astype(jnp.float32)
        slot_rows[...] = jnp.where(match > 0, before + base, -1.0)
        weight_rows[...] = weight

    def pick(step):
        level = order[step]
        if step == 0:
            number_slots()
        for tile in range(tiles):
            core_copy(level, tile, 1 - c).wait_recv()
        for b in range(CORES):
            source = pl.ds(level * CORES + b, 1)
            at = lax.broadcasted_iota(jnp.int32, (slots, rows), 0).astype(jnp.float32)
            chosen = at == slot_rows[source]
            table = jnp.where(chosen, 1.0, 0.0)
            scale[b] = jnp.sum(jnp.where(chosen, weight_rows[source], 0.0), axis=1, keepdims=True)
            spread[b] = table.T.astype(jnp.bfloat16)
            table = table.astype(jnp.bfloat16)
            squares = jnp.zeros((slots, 1), jnp.float32)
            into = slice(b * slots, (b + 1) * slots)
            for start in range(0, width, wide):
                lanes = slice(start, start + wide)
                value = jnp.dot(
                    table,
                    held[level, b * rows : (b + 1) * rows, lanes],
                    preferred_element_type=jnp.float32,
                )
                squares = squares + jnp.sum(value * value, axis=1, keepdims=True)
                picked[into, lanes] = value.astype(jnp.bfloat16)
            inverse = lax.rsqrt(squares / width + EPS)
            for start in range(0, width, wide):
                lanes = slice(start, start + wide)
                value = picked[into, lanes].astype(jnp.float32) * inverse * gain_ref[:, lanes]
                picked[into, lanes] = value.astype(jnp.bfloat16)

    def grow(step):
        for piece in range(pieces):
            if step == 0:
                gate_copy(piece, 0).wait()
                gate_copy(piece, 1).wait()
            both = jnp.dot(picked[...], gu[piece], preferred_element_type=jnp.float32)
            gate, up = both[:, :lanes_each], both[:, lanes_each:]
            lanes = slice(piece * lanes_each, (piece + 1) * lanes_each)
            hid[:, lanes] = (jax.nn.silu(gate) * up).astype(jnp.bfloat16)

    def pair_copy(level, tile):
        lanes = pl.ds(pl.multiple_of(tile * cols, cols), cols)
        return pltpu.make_async_remote_copy(
            src_ref=parts.at[level, 1 - c, :, lanes],
            dst_ref=r_pair.at[level, :, lanes],
            send_sem=p_send.at[level, tile],
            recv_sem=p_recv.at[level, tile],
            device_id=place.partner,
            device_id_type=MESH,
        )

    def shrink(step):
        level = order[step]
        if step == 0:
            down_copy.wait()
        for tile in (place.td, place.tx, place.ty, tp):
            lanes = pl.ds(pl.multiple_of(tile * cols, cols), cols)
            term = jnp.dot(hid[...], dn[:, lanes], preferred_element_type=jnp.float32)
            for b in range(CORES):
                scaled = (term[b * slots : (b + 1) * slots] * scale[b]).astype(jnp.bfloat16)
                value = jnp.dot(spread[b], scaled, preferred_element_type=jnp.float32)
                parts[level, b, :, lanes] = value.astype(jnp.bfloat16)
            pair_copy(level, tile).start()

    def summed(level, tile, row, count=chunk):
        at = pl.ds(pl.multiple_of(row, chunk), count)
        lanes = pl.ds(pl.multiple_of(tile * cols, cols), cols)
        mine = parts[level, c, at, lanes].astype(jnp.float32)
        return mine + r_pair[level, at, lanes].astype(jnp.float32)

    def over(first, last, body):
        def step(index, carry):
            body(pl.multiple_of(first + index * chunk, chunk))
            return carry

        lax.fori_loop(0, (last - first) // chunk, step, 0)

    def diag(kind, level):
        if kind == DY:
            return place.copy(kind, level, s_diag.at[level, pl.ds(0, half)], r_ydiag.at[level])
        return place.copy(kind, level, s_diag.at[level, pl.ds(half, half)], r_xdiag.at[level])

    def side(kind, level):
        source, arrived = (s_x, r_x) if kind in (X, XP) else (s_y, r_y)
        at = pl.ds(0 if kind in (X, YP) else half, half)
        return place.copy(kind, level, source.at[level, at], arrived.at[level, at])

    def owner_copy(level, part_of, arriving):
        at = pl.ds(part_of * half, half)
        return pltpu.make_async_remote_copy(
            src_ref=s_z.at[level, at],
            dst_ref=r_z.at[level if arriving else z, at],
            send_sem=z_send.at[4 + part_of, level],
            recv_sem=z_recv.at[2 + part_of, level if arriving else z],
            device_id=(level * CORES + c, tp),
            device_id_type=MESH,
        )

    def first(step):
        level = order[step]

        def plain(buffer, tile):
            def body(row):
                buffer[level, pl.ds(row, chunk)] = summed(level, tile, row).astype(jnp.bfloat16)

            return body

        pair_copy(level, place.td).wait_recv()
        over(0, half, plain(s_diag, place.td))
        diag(DY, level).start()
        over(half, rows, plain(s_diag, place.td))
        diag(DX, level).start()
        pair_copy(level, place.tx).wait_recv()
        over(half, rows, plain(s_x, place.tx))
        side(XP, level).start()
        pair_copy(level, place.ty).wait_recv()
        over(0, half, plain(s_y, place.ty))
        side(YP, level).start()

    def second(step):
        level = order[step]

        def joined(buffer, tile, arrived, base):
            def body(row):
                other = arrived[level, pl.ds(pl.multiple_of(row - base, chunk), chunk)]
                total = summed(level, tile, row) + other.astype(jnp.float32)
                buffer[level, pl.ds(row, chunk)] = total.astype(jnp.bfloat16)

            return body

        diag(DY, level).wait_recv()
        over(0, half, joined(s_x, place.tx, r_ydiag, 0))
        side(X, level).start()
        diag(DX, level).wait_recv()
        over(half, rows, joined(s_y, place.ty, r_xdiag, half))
        side(Y, level).start()

    def plane_sum(level, row):
        at = pl.ds(row, chunk)
        total = summed(level, tp, row)
        return total + r_x[level, at].astype(jnp.float32) + r_y[level, at].astype(jnp.float32)

    def plane_wait(level, part_of):
        if part_of == 0:
            pair_copy(level, tp).wait_recv()
        for kind in ((X, YP), (XP, Y))[part_of]:
            side(kind, level).wait_recv()

    def third(step):
        if step == 0:
            return
        level = order[step]

        def body(row):
            s_z[level, pl.ds(row, chunk)] = plane_sum(level, row).astype(jnp.bfloat16)

        for part_of in range(2):
            plane_wait(level, part_of)
            over(part_of * half, (part_of + 1) * half, body)
            owner_copy(level, part_of, False).start()

    def final(kind, tile, part_of):
        at = pl.ds(part_of * half, half)
        ref = out_ref.at[at, pl.ds(pl.multiple_of(tile * cols, cols), cols)]
        return place.copy(kind, part_of, ref, ref)

    def finish(step):
        level = order[step]

        def body(row):
            at = pl.ds(row, chunk)
            total = plane_sum(level, row)
            for other in order[1:]:
                total = total + r_z[other, at].astype(jnp.float32)
            total = total + own_ref[at].astype(jnp.float32)
            lanes = pl.ds(pl.multiple_of(tp * cols, cols), cols)
            out_ref[at, lanes] = total.astype(jnp.bfloat16)

        for part_of in range(2):
            plane_wait(level, part_of)
            for other in order[1:]:
                owner_copy(other, part_of, True).wait_recv()
            over(part_of * half, (part_of + 1) * half, body)
            final(FX, tp, part_of).start()
            final(FY, tp, part_of).start()

    def rim_copy(step):
        return pltpu.make_async_remote_copy(
            src_ref=rim_out,
            dst_ref=rim_in,
            send_sem=rim_send.at[0],
            recv_sem=rim_recv.at[0],
            device_id=(place.sp + step, tp),
            device_id_type=MESH,
        )

    mine = pl.ds(pl.multiple_of(tp * cols, cols), cols)

    def normalize():
        squares = jnp.zeros((rows, 1), jnp.float32)
        for start in range(0, width, cols):
            value = stream_ref[:, start : start + cols].astype(jnp.float32)
            squares = squares + jnp.sum(value * value, axis=1, keepdims=True)
        inverse = lax.rsqrt(squares / width + EPS)
        value = stream_ref[:, mine].astype(jnp.float32) * inverse * mix_ref[:, mine]
        value = value.astype(jnp.bfloat16)
        extended[SPAN:] = value.astype(jnp.float32)
        rim_out[...] = value[rows - SPAN :]

    def mix():
        extended[:SPAN] = rim_in[...].astype(jnp.float32)
        value = extended[...]
        sums, reach = value, 1
        window_sum = jnp.zeros_like(value)
        for group in range(GROUPS):
            sums = sums + pltpu.roll(sums, reach, 0)
            reach = 2 * reach
            window_sum = jnp.where(tp == group, sums, window_sum)
        position = place.sp * rows + lax.broadcasted_iota(jnp.int32, (rows, 1), 0)
        window = 2
        for group in range(1, GROUPS):
            window = jnp.where(tp == group, 2 ** (group + 1), window)
        divisor = jnp.minimum(position + 1, window).astype(jnp.float32)
        pooled = (window_sum[SPAN:] / divisor - value[SPAN:]).astype(jnp.bfloat16)
        mixed = jnp.dot(pooled, pool_ref[...], preferred_element_type=jnp.float32)
        mixed = (mixed * pool_scale_ref[...]).astype(jnp.bfloat16).astype(jnp.float32)
        after = (stream_ref[:, mine].astype(jnp.float32) + mixed).astype(jnp.bfloat16)
        own_ref[...] = after
        held[z, pl.ds(pl.multiple_of(c * rows, rows), rows), mine] = after

    for piece in range(pieces):
        gate_copy(piece, 0).start()
        gate_copy(piece, 1).start()
    down_copy.start()
    normalize()
    meta_ref[...] = jnp.zeros_like(meta_ref)
    meta_ref[0:TOP_K] = ids_ref[...].astype(jnp.float32)
    meta_ref[TOP_K : 2 * TOP_K] = shares_ref[...]
    local_meta = pltpu.make_async_copy(meta_ref, metas.at[place.sp], l_sem.at[0])
    local_meta.start()
    pl.when(place.sp == 0)(lambda: rim_in.__setitem__(Ellipsis, jnp.zeros_like(rim_in)))
    local_meta.wait()
    greet(place)
    pl.when(place.sp < sp_count - 1)(lambda: rim_copy(1).start())
    for hop in range(1, sp_count):
        meta_copy(hop).start()
    pl.when(place.sp > 0)(lambda: rim_copy(-1).wait_recv())
    mix()
    line_own(0, lambda copy: copy.start())

    stages = {
        "relay": lambda step: line_relay(step, 0),
        "relay_diagonal": lambda step: line_relay(step, 1),
        "spread_line": spread_line,
        "spread_diagonal": spread_diagonal,
        "spread_last": spread_last,
        "pick": pick,
        "grow": grow,
        "shrink": shrink,
        "first": first,
        "second": second,
        "third": third,
        "finish": finish,
    }
    for stage, step in schedule(place.levels):
        stages[stage](step)

    final(FX, place.tx, 0).wait_recv()
    final(FDY, place.tx, 0).start()
    final(FY, place.ty, 0).wait_recv()
    final(FY, place.ty, 1).wait_recv()
    final(FDX, place.ty, 1).start()
    final(FX, place.tx, 1).wait_recv()
    for hop in range(1, sp_count):
        meta_copy(hop).wait_send()
    pl.when(place.sp < sp_count - 1)(lambda: rim_copy(1).wait_send())
    line_own(0, lambda copy: copy.wait_send())
    line_own(1, lambda copy: copy.wait_send())
    for step, level in enumerate(order):
        whole(GX, level, tp).wait_send()
        whole(GY, level, tp).wait_send()
        for tile in range(tiles):
            core_copy(level, tile, c).wait_send()
            pair_copy(level, tile).wait_send()
        for kind in (DX, DY):
            diag(kind, level).wait_send()
        for kind in (X, Y, XP, YP):
            side(kind, level).wait_send()
        if step:
            for part_of in range(2):
                line_on(level, part_of, lambda copy: copy.wait_send())
                owner_copy(level, part_of, False).wait_send()
        else:
            part(GDY, level, place.tx).wait_send()
            part(GDX, level, place.ty).wait_send()
    final(FDY, place.td, 0).wait_recv()
    final(FDX, place.td, 1).wait_recv()
    for part_of in range(2):
        final(FX, tp, part_of).wait_send()
        final(FY, tp, part_of).wait_send()
    final(FDY, place.tx, 0).wait_send()
    final(FDX, place.ty, 1).wait_send()


def layer_all(
    stream, mix_gain, pool, pool_scale, ids, shares, gain, gate, up, down, capacity, sp_count, tp_count
):
    rows, cols = stream.shape[0], pool.shape[1]
    width = tp_count * cols
    hidden = gate.shape[2]
    levels = sp_count // CORES
    slots = capacity * tp_count
    vmem = pl.BlockSpec(memory_space=pltpu.VMEM)
    hbm = pl.BlockSpec(memory_space=pl.ANY)
    whole = pltpu.VMEM((levels, rows, cols), jnp.bfloat16)
    halved = pltpu.VMEM((levels, rows // 2, cols), jnp.bfloat16)
    pieces = hidden // LANES
    return pl.pallas_call(
        layer_kernel,
        out_shape=jax.ShapeDtypeStruct((rows, width), stream.dtype),
        in_specs=[vmem, vmem, vmem, vmem, vmem, vmem, vmem, hbm, hbm, hbm],
        out_specs=vmem,
        scratch_shapes=[
            pltpu.VMEM((rows, cols), jnp.bfloat16),
            pltpu.VMEM((SPAN + rows, cols), jnp.float32),
            pltpu.VMEM((SPAN, cols), jnp.bfloat16),
            pltpu.VMEM((SPAN, cols), jnp.bfloat16),
            pltpu.VMEM((8, rows), jnp.float32),
            pltpu.VMEM((levels, CORES * rows, width), jnp.bfloat16),
            pltpu.VMEM((sp_count, 8, rows), jnp.float32),
            pltpu.VMEM((sp_count, rows), jnp.float32),
            pltpu.VMEM((sp_count, rows), jnp.float32),
            pltpu.VMEM((pieces, width, 2 * LANES), jnp.bfloat16),
            pltpu.VMEM((hidden, width), jnp.bfloat16),
            pltpu.VMEM((CORES * slots, width), jnp.bfloat16),
            pltpu.VMEM((CORES * slots, hidden), jnp.bfloat16),
            pltpu.VMEM((CORES, rows, slots), jnp.bfloat16),
            pltpu.VMEM((CORES, slots, 1), jnp.float32),
            pltpu.VMEM((levels, CORES, rows, width), jnp.bfloat16),
            pltpu.VMEM((levels, rows, width), jnp.bfloat16),
            whole, halved, halved, whole, whole, whole, whole, whole, whole,
            pltpu.SemaphoreType.DMA((KINDS, max(2, levels))),
            pltpu.SemaphoreType.DMA((KINDS, max(2, levels))),
            pltpu.SemaphoreType.DMA((levels, tp_count)),
            pltpu.SemaphoreType.DMA((levels, tp_count)),
            pltpu.SemaphoreType.DMA((levels, tp_count)),
            pltpu.SemaphoreType.DMA((levels, tp_count)),
            pltpu.SemaphoreType.DMA((6, levels)),
            pltpu.SemaphoreType.DMA((4, levels)),
            pltpu.SemaphoreType.DMA((sp_count,)),
            pltpu.SemaphoreType.DMA((sp_count,)),
            pltpu.SemaphoreType.DMA((pieces + 1, 2)),
            pltpu.SemaphoreType.DMA((1,)),
            pltpu.SemaphoreType.DMA((1,)),
            pltpu.SemaphoreType.DMA((1,)),
        ],
        compiler_params=pltpu.CompilerParams(
            collective_id=0, has_side_effects=True, vmem_limit_bytes=62 * 1024 * 1024
        ),
        name="layer_all",
    )(stream, mix_gain, pool, pool_scale, ids, shares, gain, gate, up, down)


def shards(
    residual_in,
    mix_gain,
    pool_weight,
    pool_scale,
    ffn_gain,
    route_ids,
    route_weights,
    gate_weight,
    up_weight,
    down_weight,
):
    tp_count = lax.axis_size("tp")
    sp_count = lax.axis_size("sp")
    block_rows = residual_in.shape[0] // tp_count
    return layer_all(
        residual_in,
        mix_gain[None],
        pool_weight,
        pool_scale[None],
        route_ids.T,
        route_weights.T,
        ffn_gain[None],
        gate_weight,
        up_weight,
        down_weight,
        2 * TOP_K * block_rows // sp_count,
        sp_count,
        tp_count,
    )


def solution(mesh):
    placed = (
        P("sp", None),
        P(),
        P(None, "tp"),
        P("tp"),
        P(),
        P("sp", None),
        P("sp", None),
        P("sp", None, "tp"),
        P("sp", None, "tp"),
        P("sp", "tp", None),
    )
    square = mesh.shape["tp"] == SIDE * SIDE and mesh.shape["sp"] % CORES == 0
    return jax.shard_map(
        shards if square else shards_any,
        mesh=mesh,
        in_specs=placed,
        out_specs=P("sp", None),
        check_vma=False,
    )
```

```python
import jax
import jax.numpy as jnp
from jax import lax
from jax.experimental import pallas as pl
from jax.experimental.pallas import tpu as pltpu
from jax.sharding import PartitionSpec as P

GROUPS = 4
SPAN = 16
TOP_K = 2
CORES = 2
SIDE = 2
LANES = 128
EPS = 1e-06
MESH = pl.DeviceIdType.MESH
KINDS = 16
X, Y, DX, DY, XP, YP, FX, FY, FDX, FDY, GX, GY, GDX, GDY, GXH, GYH = range(KINDS)

def from_behind(value, axis, steps):
    count = lax.axis_size(axis)
    first, last = (max(0, -steps), min(count, count - steps))
    return lax.ppermute(value, axis, [(source, source + steps) for source in range(first, last)])


def rms_scale(values, gain):
    return values * lax.rsqrt(jnp.mean(values * values, axis=-1, keepdims=True) + EPS) * gain


def slot_table(chosen_ids, experts, capacity):
    flat_ids = chosen_ids.reshape(-1)
    matches = (flat_ids[:, None] == jnp.arange(experts, dtype=jnp.int32)[None, :]).astype(jnp.int32)
    before = jnp.cumsum(matches, axis=0) - matches
    slot_of = jnp.sum(before * matches, axis=1)
    target = flat_ids * capacity + slot_of
    return (target[:, None] == jnp.arange(experts * capacity, dtype=jnp.int32)[None, :]).astype(
        jnp.float32
    )


def shards_any(
    residual_in,
    mix_gain,
    pool_weight,
    pool_scale,
    ffn_gain,
    route_ids,
    route_weights,
    gate_weight,
    up_weight,
    down_weight,
):
    tp_count = lax.axis_size("tp")
    sp_count = lax.axis_size("sp")
    tp_index = lax.axis_index("tp")
    tok_count, width = residual_in.shape
    group_width = width // GROUPS
    col_count = pool_weight.shape[1]
    row_count = tok_count // tp_count
    capacity = 2 * TOP_K * row_count // sp_count
    group_index = tp_index * col_count // group_width
    window = jnp.power(2, group_index + 1)
    stream = residual_in.astype(jnp.float32)
    inverse = lax.rsqrt(jnp.mean(stream * stream, axis=-1, keepdims=True) + EPS)
    stream_group = lax.dynamic_slice_in_dim(stream, group_index * group_width, group_width, 1)
    gain_group = lax.dynamic_slice_in_dim(mix_gain, group_index * group_width, group_width, 0)
    normed_group = (stream_group * inverse * gain_group).astype(jnp.bfloat16)
    rim_rows = from_behind(normed_group[tok_count - SPAN :], "sp", 1)
    extended = jnp.concatenate([rim_rows, normed_group], axis=0).astype(jnp.float32)
    window_sum = jnp.zeros((tok_count, group_width), jnp.float32)
    for offset in range(SPAN):
        window_sum = window_sum + jnp.where(
            offset < window, extended[SPAN - offset : SPAN - offset + tok_count], 0.0
        )
    position = lax.axis_index("sp") * tok_count + jnp.arange(tok_count, dtype=jnp.int32)
    divisor = jnp.minimum(position + 1, window).astype(jnp.float32)
    pooled = (window_sum / divisor[:, None] - extended[SPAN:]).astype(jnp.bfloat16)
    mixed = (jnp.dot(pooled, pool_weight, preferred_element_type=jnp.float32) * pool_scale).astype(
        jnp.bfloat16
    )
    stream_own = lax.dynamic_slice_in_dim(stream, tp_index * row_count, row_count, 0)
    mixed_own = lax.all_to_all(mixed, "tp", split_axis=0, concat_axis=1, tiled=True)
    after_own = (stream_own + mixed_own.astype(jnp.float32)).astype(jnp.bfloat16)
    normed_own = rms_scale(after_own.astype(jnp.float32), ffn_gain).astype(jnp.bfloat16)
    ids_own = lax.dynamic_slice_in_dim(route_ids, tp_index * row_count, row_count, 0)
    table_own = slot_table(ids_own, sp_count, capacity)
    repeated = jnp.repeat(normed_own, TOP_K, axis=0)
    outgoing = lax.dot_general(
        table_own.astype(jnp.bfloat16),
        repeated,
        (((0,), (0,)), ((), ())),
        preferred_element_type=jnp.float32,
    )
    outgoing = outgoing.astype(jnp.bfloat16).reshape(sp_count, capacity, width)
    arrived = lax.all_to_all(outgoing, "sp", split_axis=0, concat_axis=0, tiled=True)
    piece = lax.all_gather(arrived, "tp", axis=0, tiled=True)
    flat_rows = piece.reshape(-1, width)
    gate_part = jnp.dot(flat_rows, gate_weight[0], preferred_element_type=jnp.float32)
    up_part = jnp.dot(flat_rows, up_weight[0], preferred_element_type=jnp.float32)
    hidden = (jax.nn.silu(gate_part) * up_part).astype(jnp.bfloat16)
    hidden_all = hidden.reshape(piece.shape[0], piece.shape[1], hidden.shape[1])
    hidden_flat = hidden_all.reshape(-1, hidden_all.shape[-1])
    term = jnp.dot(hidden_flat, down_weight[0], preferred_element_type=jnp.float32)
    summed = lax.psum_scatter(
        term.astype(jnp.bfloat16).astype(jnp.float32).astype(jnp.bfloat16),
        "tp",
        scatter_dimension=0,
        tiled=True,
    )
    expert_out = summed.reshape(sp_count, capacity, width)
    returned_rows = lax.all_to_all(expert_out, "sp", split_axis=0, concat_axis=0, tiled=True)
    weights_own = lax.dynamic_slice_in_dim(route_weights, tp_index * row_count, row_count, 0)
    weight_table = jnp.einsum(
        "rk,rkc->rc", weights_own, table_own.reshape(row_count, TOP_K, sp_count * capacity)
    )
    expert_mix = jnp.dot(
        weight_table,
        returned_rows.reshape(-1, width).astype(jnp.float32),
        precision=lax.Precision.HIGHEST,
    )
    out_own = (after_own.astype(jnp.float32) + expert_mix).astype(jnp.bfloat16)
    return lax.all_gather(out_own, "tp", axis=0, tiled=True)


class Place:
    def __init__(self, send_sem, recv_sem):
        self.sp, self.tp = lax.axis_index("sp"), lax.axis_index("tp")
        self.levels = lax.axis_size("sp") // CORES
        self.z, self.c = self.sp // CORES, self.sp % CORES
        y, x = self.tp // SIDE, self.tp % SIDE
        self.tx = y * SIDE + (1 - x)
        self.ty = (1 - y) * SIDE + x
        self.td = (1 - y) * SIDE + (1 - x)
        self.send_sem, self.recv_sem = send_sem, recv_sem
        partner = self.z * CORES + (1 - self.c)
        self.partner = (partner, self.tp)
        along_x, along_y = (self.sp, self.tx), (self.sp, self.ty)
        self.to = {kind: along_x for kind in (X, XP, DX, FX, FDX, GX, GDX, GXH)}
        self.to.update({kind: along_y for kind in (Y, YP, DY, FY, FDY, GY, GDY, GYH)})

    def copy(self, kind, index, src, dst):
        return pltpu.make_async_remote_copy(
            src_ref=src,
            dst_ref=dst,
            send_sem=self.send_sem.at[kind, index],
            recv_sem=self.recv_sem.at[kind, index],
            device_id=self.to[kind],
            device_id_type=MESH,
        )

    def offsets(self):
        order = [0]
        for distance in range(1, self.levels):
            order += [-distance, distance]
        return order


def greet(place):
    barrier = pltpu.get_barrier_semaphore()

    def hello(target):
        pl.semaphore_signal(barrier, inc=1, device_id=target, device_id_type=MESH)

    count = lax.axis_size("sp")
    hello(place.to[X])
    hello(place.to[Y])
    for step in range(1, count):
        hello((lax.rem(place.sp + step, count), place.tp))
    return lambda: pl.semaphore_wait(barrier, count + 1)


def level_order(place):
    everywhere = range(place.levels)
    orders = []
    for z in everywhere:
        offsets = [offset for offset in place.offsets() if 0 <= z + offset < place.levels]
        orders.append([z + offset for offset in offsets])
    steps = []
    for index in everywhere:
        level = jnp.int32(orders[0][index])
        for z in everywhere[1:]:
            level = jnp.where(place.z == z, orders[z][index], level)
        steps.append(level)
    return steps


PLAN = [
    ("spread_line", 0), ("spread_diagonal", 0), ("relay", 2), ("relay", 1), ("relay_rest", 1),
    ("relay_rest", 2), ("spread_line", 1), ("spread_last", 0), ("pick", 0), ("spread_line", 2),
    ("relay", 3), ("grow", 0), ("shrink", 0), ("relay_rest", 3), ("relay_diagonal", 2),
    ("first", 0), ("relay_diagonal_rest", 2), ("spread_diagonal", 2), ("relay_diagonal", 1),
    ("spread_diagonal", 1), ("relay_diagonal_rest", 1), ("spread_last", 1), ("spread_line", 3),
    ("pick", 1), ("grow", 1), ("relay_diagonal", 3), ("shrink", 1), ("relay_diagonal_rest", 3),
    ("spread_last", 2), ("first", 1), ("pick", 2), ("grow", 2), ("shrink", 2), ("second", 1),
    ("spread_diagonal", 3), ("spread_last", 3), ("first", 2), ("pick", 3), ("grow", 3),
    ("shrink", 3), ("third", 1), ("second", 2), ("first", 3), ("third", 2), ("second", 3),
    ("third", 3), ("second", 0), ("finish", 0),
]


def schedule(levels):
    if levels == 1 + max(step for _, step in PLAN):
        return PLAN
    plan = []
    for turn in range(levels + 3):
        step = turn - 2
        plan += [("relay", turn), ("relay_rest", turn)]
        plan += [("relay_diagonal", step), ("relay_diagonal_rest", step)]
        plan += [("spread_line", turn), ("spread_diagonal", turn - 1), ("spread_last", step)]
        plan += [("pick", step), ("first", step - 1), ("grow", step), ("second", step - 2)]
        plan += [("shrink", step), ("third", step - 3)]
    plan += [("second", levels - 1), ("third", levels - 2), ("third", levels - 1), ("finish", 0)]
    return [(stage, step) for stage, step in plan if 0 <= step < levels]


def layer_kernel(
    stream_ref, mix_ref, pool_ref, pool_scale_ref, ids_ref, shares_ref,
    gain_ref, gate_ref, up_ref, down_ref, out_ref,
    own_ref, extended, rim_out, rim_in, meta_ref, held, metas, slot_rows, weight_rows, gu, dn, picked, hid, spread, scale, parts,
    r_pair, s_diag, r_ydiag, r_xdiag, s_x, s_y, r_x, r_y, s_z, r_z,
    send_sem, recv_sem, g_send, g_recv, p_send, p_recv, z_send, z_recv, m_send, m_recv,
    w_sem, l_sem, rim_send, rim_recv,
):
    place = Place(send_sem, recv_sem)
    rows, cols = own_ref.shape
    width = held.shape[2]
    slots = spread.shape[2]
    sp_count, tiles = lax.axis_size("sp"), SIDE * SIDE
    half = rows // 2
    z, c, tp = place.z, place.c, place.tp
    chunk, wide = 32, 256
    pieces, _, pair_lanes = gu.shape
    lanes_each = pair_lanes // 2
    order = level_order(place)

    def gate_copy(piece, side):
        source = (gate_ref, up_ref)[side]
        return pltpu.make_async_copy(
            source.at[0, :, pl.ds(piece * lanes_each, lanes_each)],
            gu.at[piece, :, pl.ds(side * lanes_each, lanes_each)],
            w_sem.at[piece, side],
        )

    down_copy = pltpu.make_async_copy(down_ref.at[0], dn, w_sem.at[pieces, 0])

    def block(level, core, tile, first=0, count=rows):
        at = pl.ds(pl.multiple_of(core * rows + first, half), count)
        return held.at[level, at, pl.ds(pl.multiple_of(tile * cols, cols), cols)]

    def meta_copy(step):
        return pltpu.make_async_remote_copy(
            src_ref=meta_ref,
            dst_ref=metas.at[place.sp],
            send_sem=m_send.at[step],
            recv_sem=m_recv.at[step],
            device_id=(lax.rem(place.sp + step, sp_count), tp),
            device_id_type=MESH,
        )

    middle = (z > 0) & (z < place.levels - 1)
    has_up, has_down = z < place.levels - 1, z > 0

    def line(level, diagonal, part_of, up=True):
        ref = block(level, c, place.td if diagonal else tp, part_of * half, half)
        lane = 2 * diagonal + part_of
        return pltpu.make_async_remote_copy(
            src_ref=ref,
            dst_ref=ref,
            send_sem=z_send.at[2 * lane + up, level],
            recv_sem=z_recv.at[lane, level],
            device_id=((z + 1 if up else z - 1) * CORES + c, tp),
            device_id_type=MESH,
        )

    def line_own(diagonal, act):
        for part_of in range(2):
            pl.when(has_up)(lambda: act(line(z, diagonal, part_of, True)))
            pl.when(has_down)(lambda: act(line(z, diagonal, part_of, False)))

    def line_on(level, diagonal, part_of, act):
        pl.when(middle & (level < z))(lambda: act(line(level, diagonal, part_of, True)))
        pl.when(middle & (level > z))(lambda: act(line(level, diagonal, part_of, False)))

    def line_relay(step, diagonal, part_of):
        level = order[step]
        if step:
            pl.when(middle)(lambda: line(level, diagonal, part_of).wait_recv())
            line_on(level, diagonal, part_of, lambda copy: copy.start())

    def line_end(level, diagonal):
        for part_of in range(2):
            pl.when(jnp.logical_not(middle))(lambda: line(level, diagonal, part_of).wait_recv())

    def core_copy(level, tile, core):
        ref = block(level, core, tile)
        return pltpu.make_async_remote_copy(
            src_ref=ref,
            dst_ref=ref,
            send_sem=g_send.at[level, tile],
            recv_sem=g_recv.at[level, tile],
            device_id=place.partner,
            device_id_type=MESH,
        )

    def whole(kind, level, tile):
        ref = block(level, c, tile)
        return place.copy(kind, level, ref, ref)

    def part(kind, level, tile):
        ref = block(level, c, tile, 0 if kind == GDY else half, half)
        return place.copy(kind, level, ref, ref)

    def own_half(kind, tile, part_of):
        ref = block(z, c, tile, part_of * half, half)
        return place.copy(kind, part_of, ref, ref)

    def spread_line(step):
        level = order[step]
        if step:
            line_end(level, 0)
            whole(GX, level, tp).start()
            whole(GY, level, tp).start()
        else:
            for part_of in range(2):
                own_half(GXH, tp, part_of).start()
                own_half(GYH, tp, 1 - part_of).start()
        core_copy(level, tp, c).start()

    def spread_diagonal(step):
        level = order[step]
        if step:
            whole(GX, level, place.tx).wait_recv()
            core_copy(level, place.tx, c).start()
            whole(GY, level, place.ty).wait_recv()
            core_copy(level, place.ty, c).start()
        else:
            own_half(GXH, place.tx, 0).wait_recv()
            part(GDY, level, place.tx).start()
            own_half(GYH, place.ty, 1).wait_recv()
            part(GDX, level, place.ty).start()

    def spread_last(step):
        level = order[step]
        if step:
            line_end(level, 1)
        else:
            own_half(GXH, place.tx, 1).wait_recv()
            core_copy(level, place.tx, c).start()
            own_half(GYH, place.ty, 0).wait_recv()
            core_copy(level, place.ty, c).start()
            part(GDY, level, place.td).wait_recv()
            part(GDX, level, place.td).wait_recv()
            line_own(1, lambda copy: copy.start())
        core_copy(level, place.td, c).start()

    def number_slots():
        for hop in range(1, sp_count):
            meta_copy(hop).wait_recv()
        expert = place.sp.astype(jnp.float32)
        match = jnp.zeros((sp_count, rows), jnp.float32)
        weight = jnp.zeros((sp_count, rows), jnp.float32)
        for k in range(TOP_K):
            named = jnp.where(metas[:, k] == expert, 1.0, 0.0)
            match = match + named
            weight = weight + named * metas[:, TOP_K + k]
        block_rows = rows // tiles
        source = lax.broadcasted_iota(jnp.int32, (rows, rows), 0)
        target = lax.broadcasted_iota(jnp.int32, (rows, rows), 1)
        earlier = (source < target) & (source // block_rows == target // block_rows)
        earlier = jnp.where(earlier, 1.0, 0.0).astype(jnp.bfloat16)
        before = jnp.dot(match.astype(jnp.bfloat16), earlier, preferred_element_type=jnp.float32)
        at = lax.broadcasted_iota(jnp.int32, (sp_count, rows), 1)
        base = (at // block_rows * (slots // tiles)).astype(jnp.float32)
        slot_rows[...] = jnp.where(match > 0, before + base, -1.0)
        weight_rows[...] = weight

    def pick(step):
        level = order[step]
        if step == 0:
            number_slots()
        for tile in range(tiles):
            core_copy(level, tile, 1 - c).wait_recv()
        for b in range(CORES):
            source = pl.ds(level * CORES + b, 1)
            at = lax.broadcasted_iota(jnp.int32, (slots, rows), 0).astype(jnp.float32)
            chosen = at == slot_rows[source]
            table = jnp.where(chosen, 1.0, 0.0)
            scale[b] = jnp.sum(jnp.where(chosen, weight_rows[source], 0.0), axis=1, keepdims=True)
            spread[b] = table.T.astype(jnp.bfloat16)
            table = table.astype(jnp.bfloat16)
            squares = jnp.zeros((slots, 1), jnp.float32)
            into = slice(b * slots, (b + 1) * slots)
            for start in range(0, width, wide):
                lanes = slice(start, start + wide)
                value = jnp.dot(
                    table,
                    held[level, b * rows : (b + 1) * rows, lanes],
                    preferred_element_type=jnp.float32,
                )
                squares = squares + jnp.sum(value * value, axis=1, keepdims=True)
                picked[into, lanes] = value.astype(jnp.bfloat16)
            inverse = lax.rsqrt(squares / width + EPS)
            for start in range(0, width, wide):
                lanes = slice(start, start + wide)
                value = picked[into, lanes].astype(jnp.float32) * inverse * gain_ref[:, lanes]
                picked[into, lanes] = value.astype(jnp.bfloat16)

    def grow(step):
        for piece in range(pieces):
            if step == 0:
                gate_copy(piece, 0).wait()
                gate_copy(piece, 1).wait()
            both = jnp.dot(picked[...], gu[piece], preferred_element_type=jnp.float32)
            gate, up = both[:, :lanes_each], both[:, lanes_each:]
            lanes = slice(piece * lanes_each, (piece + 1) * lanes_each)
            hid[:, lanes] = (jax.nn.silu(gate) * up).astype(jnp.bfloat16)

    def pair_copy(level, tile):
        lanes = pl.ds(pl.multiple_of(tile * cols, cols), cols)
        return pltpu.make_async_remote_copy(
            src_ref=parts.at[level, 1 - c, :, lanes],
            dst_ref=r_pair.at[level, :, lanes],
            send_sem=p_send.at[level, tile],
            recv_sem=p_recv.at[level, tile],
            device_id=place.partner,
            device_id_type=MESH,
        )

    def shrink(step):
        level = order[step]
        if step == 0:
            down_copy.wait()
        for tile in (place.td, place.tx, place.ty, tp):
            lanes = pl.ds(pl.multiple_of(tile * cols, cols), cols)
            term = jnp.dot(hid[...], dn[:, lanes], preferred_element_type=jnp.float32)
            for b in range(CORES):
                scaled = (term[b * slots : (b + 1) * slots] * scale[b]).astype(jnp.bfloat16)
                value = jnp.dot(spread[b], scaled, preferred_element_type=jnp.float32)
                parts[level, b, :, lanes] = value.astype(jnp.bfloat16)
            pair_copy(level, tile).start()

    def summed(level, tile, row, count=chunk):
        at = pl.ds(pl.multiple_of(row, chunk), count)
        lanes = pl.ds(pl.multiple_of(tile * cols, cols), cols)
        mine = parts[level, c, at, lanes].astype(jnp.float32)
        return mine + r_pair[level, at, lanes].astype(jnp.float32)

    def over(first, last, body):
        def step(index, carry):
            body(pl.multiple_of(first + index * chunk, chunk))
            return carry

        lax.fori_loop(0, (last - first) // chunk, step, 0)

    def diag(kind, level):
        if kind == DY:
            return place.copy(kind, level, s_diag.at[level, pl.ds(0, half)], r_ydiag.at[level])
        return place.copy(kind, level, s_diag.at[level, pl.ds(half, half)], r_xdiag.at[level])

    def side(kind, level):
        source, arrived = (s_x, r_x) if kind in (X, XP) else (s_y, r_y)
        at = pl.ds(0 if kind in (X, YP) else half, half)
        return place.copy(kind, level, source.at[level, at], arrived.at[level, at])

    def owner_copy(level, part_of, arriving):
        at = pl.ds(part_of * half, half)
        return pltpu.make_async_remote_copy(
            src_ref=s_z.at[level, at],
            dst_ref=r_z.at[level if arriving else z, at],
            send_sem=z_send.at[8 + part_of, level],
            recv_sem=z_recv.at[4 + part_of, level if arriving else z],
            device_id=(level * CORES + c, tp),
            device_id_type=MESH,
        )

    def first(step):
        level = order[step]

        def plain(buffer, tile):
            def body(row):
                buffer[level, pl.ds(row, chunk)] = summed(level, tile, row).astype(jnp.bfloat16)

            return body

        pair_copy(level, place.td).wait_recv()
        over(0, half, plain(s_diag, place.td))
        diag(DY, level).start()
        over(half, rows, plain(s_diag, place.td))
        diag(DX, level).start()
        pair_copy(level, place.tx).wait_recv()
        over(half, rows, plain(s_x, place.tx))
        side(XP, level).start()
        pair_copy(level, place.ty).wait_recv()
        over(0, half, plain(s_y, place.ty))
        side(YP, level).start()

    def second(step):
        level = order[step]

        def joined(buffer, tile, arrived, base):
            def body(row):
                other = arrived[level, pl.ds(pl.multiple_of(row - base, chunk), chunk)]
                total = summed(level, tile, row) + other.astype(jnp.float32)
                buffer[level, pl.ds(row, chunk)] = total.astype(jnp.bfloat16)

            return body

        diag(DY, level).wait_recv()
        over(0, half, joined(s_x, place.tx, r_ydiag, 0))
        side(X, level).start()
        diag(DX, level).wait_recv()
        over(half, rows, joined(s_y, place.ty, r_xdiag, half))
        side(Y, level).start()

    def plane_sum(level, row):
        at = pl.ds(row, chunk)
        total = summed(level, tp, row)
        return total + r_x[level, at].astype(jnp.float32) + r_y[level, at].astype(jnp.float32)

    def plane_wait(level, part_of):
        if part_of == 0:
            pair_copy(level, tp).wait_recv()
        for kind in ((X, YP), (XP, Y))[part_of]:
            side(kind, level).wait_recv()

    def third(step):
        if step == 0:
            return
        level = order[step]

        def body(row):
            s_z[level, pl.ds(row, chunk)] = plane_sum(level, row).astype(jnp.bfloat16)

        for part_of in range(2):
            plane_wait(level, part_of)
            over(part_of * half, (part_of + 1) * half, body)
            owner_copy(level, part_of, False).start()

    def final(kind, tile, part_of):
        at = pl.ds(part_of * half, half)
        ref = out_ref.at[at, pl.ds(pl.multiple_of(tile * cols, cols), cols)]
        return place.copy(kind, part_of, ref, ref)

    def finish(step):
        level = order[step]

        def body(row):
            at = pl.ds(row, chunk)
            total = plane_sum(level, row)
            for other in order[1:]:
                total = total + r_z[other, at].astype(jnp.float32)
            total = total + own_ref[at].astype(jnp.float32)
            lanes = pl.ds(pl.multiple_of(tp * cols, cols), cols)
            out_ref[at, lanes] = total.astype(jnp.bfloat16)

        for part_of in range(2):
            plane_wait(level, part_of)
            for other in order[1:]:
                owner_copy(other, part_of, True).wait_recv()
            over(part_of * half, (part_of + 1) * half, body)
            final(FX, tp, part_of).start()
            final(FY, tp, part_of).start()

    def rim_copy(step):
        return pltpu.make_async_remote_copy(
            src_ref=rim_out,
            dst_ref=rim_in,
            send_sem=rim_send.at[0],
            recv_sem=rim_recv.at[0],
            device_id=(place.sp + step, tp),
            device_id_type=MESH,
        )

    mine = pl.ds(pl.multiple_of(tp * cols, cols), cols)

    def normalize():
        squares = jnp.zeros((rows, 1), jnp.float32)
        for start in range(0, width, cols):
            value = stream_ref[:, start : start + cols].astype(jnp.float32)
            squares = squares + jnp.sum(value * value, axis=1, keepdims=True)
        inverse = lax.rsqrt(squares / width + EPS)
        value = stream_ref[:, mine].astype(jnp.float32) * inverse * mix_ref[:, mine]
        value = value.astype(jnp.bfloat16)
        extended[SPAN:] = value.astype(jnp.float32)
        rim_out[...] = value[rows - SPAN :]

    def mix(begin, end):
        value = extended[begin : SPAN + end]
        sums, reach = value, 1
        window_sum = jnp.zeros_like(value)
        for group in range(GROUPS):
            sums = sums + pltpu.roll(sums, reach, 0)
            reach = 2 * reach
            window_sum = jnp.where(tp == group, sums, window_sum)
        count = end - begin
        position = place.sp * rows + begin + lax.broadcasted_iota(jnp.int32, (count, 1), 0)
        window = 2
        for group in range(1, GROUPS):
            window = jnp.where(tp == group, 2 ** (group + 1), window)
        divisor = jnp.minimum(position + 1, window).astype(jnp.float32)
        pooled = (window_sum[SPAN:] / divisor - value[SPAN:]).astype(jnp.bfloat16)
        mixed = jnp.dot(pooled, pool_ref[...], preferred_element_type=jnp.float32)
        mixed = (mixed * pool_scale_ref[...]).astype(jnp.bfloat16).astype(jnp.float32)
        after = (stream_ref[begin:end, mine].astype(jnp.float32) + mixed).astype(jnp.bfloat16)
        own_ref[begin:end] = after
        held[z, pl.ds(pl.multiple_of(c * rows + begin, SPAN), count), mine] = after

    greeted = greet(place)
    for piece in range(pieces):
        gate_copy(piece, 0).start()
        gate_copy(piece, 1).start()
    down_copy.start()
    normalize()
    meta_ref[...] = jnp.zeros_like(meta_ref)
    meta_ref[0:TOP_K] = ids_ref[...].astype(jnp.float32)
    meta_ref[TOP_K : 2 * TOP_K] = shares_ref[...]
    local_meta = pltpu.make_async_copy(meta_ref, metas.at[place.sp], l_sem.at[0])
    local_meta.start()
    pl.when(place.sp == 0)(lambda: rim_in.__setitem__(Ellipsis, jnp.zeros_like(rim_in)))
    local_meta.wait()
    greeted()
    pl.when(place.sp < sp_count - 1)(lambda: rim_copy(1).start())
    for hop in range(1, sp_count):
        meta_copy(hop).start()
    mix(SPAN, rows)
    pl.when(place.sp > 0)(lambda: rim_copy(-1).wait_recv())
    extended[:SPAN] = rim_in[...].astype(jnp.float32)
    mix(0, SPAN)
    line_own(0, lambda copy: copy.start())

    stages = {
        "relay": lambda step: line_relay(step, 0, 0),
        "relay_rest": lambda step: line_relay(step, 0, 1),
        "relay_diagonal": lambda step: line_relay(step, 1, 0),
        "relay_diagonal_rest": lambda step: line_relay(step, 1, 1),
        "spread_line": spread_line,
        "spread_diagonal": spread_diagonal,
        "spread_last": spread_last,
        "pick": pick,
        "grow": grow,
        "shrink": shrink,
        "first": first,
        "second": second,
        "third": third,
        "finish": finish,
    }
    for stage, step in schedule(place.levels):
        stages[stage](step)

    final(FX, place.tx, 0).wait_recv()
    final(FDY, place.tx, 0).start()
    final(FY, place.ty, 0).wait_recv()
    final(FY, place.ty, 1).wait_recv()
    final(FDX, place.ty, 1).start()
    final(FX, place.tx, 1).wait_recv()
    for hop in range(1, sp_count):
        meta_copy(hop).wait_send()
    pl.when(place.sp < sp_count - 1)(lambda: rim_copy(1).wait_send())
    line_own(0, lambda copy: copy.wait_send())
    line_own(1, lambda copy: copy.wait_send())
    for step, level in enumerate(order):
        for tile in range(tiles):
            core_copy(level, tile, c).wait_send()
            pair_copy(level, tile).wait_send()
        for kind in (DX, DY):
            diag(kind, level).wait_send()
        for kind in (X, Y, XP, YP):
            side(kind, level).wait_send()
        if step:
            for part_of in range(2):
                line_on(level, 0, part_of, lambda copy: copy.wait_send())
                line_on(level, 1, part_of, lambda copy: copy.wait_send())
                owner_copy(level, part_of, False).wait_send()
            whole(GX, level, tp).wait_send()
            whole(GY, level, tp).wait_send()
        else:
            for part_of in range(2):
                own_half(GXH, tp, part_of).wait_send()
                own_half(GYH, tp, part_of).wait_send()
            part(GDY, level, place.tx).wait_send()
            part(GDX, level, place.ty).wait_send()
    final(FDY, place.td, 0).wait_recv()
    final(FDX, place.td, 1).wait_recv()
    for part_of in range(2):
        final(FX, tp, part_of).wait_send()
        final(FY, tp, part_of).wait_send()
    final(FDY, place.tx, 0).wait_send()
    final(FDX, place.ty, 1).wait_send()


def layer_all(
    stream, mix_gain, pool, pool_scale, ids, shares, gain, gate, up, down, capacity, sp_count, tp_count
):
    rows, cols = stream.shape[0], pool.shape[1]
    width = tp_count * cols
    hidden = gate.shape[2]
    levels = sp_count // CORES
    slots = capacity * tp_count
    vmem = pl.BlockSpec(memory_space=pltpu.VMEM)
    hbm = pl.BlockSpec(memory_space=pl.ANY)
    whole = pltpu.VMEM((levels, rows, cols), jnp.bfloat16)
    halved = pltpu.VMEM((levels, rows // 2, cols), jnp.bfloat16)
    pieces = hidden // LANES
    return pl.pallas_call(
        layer_kernel,
        out_shape=jax.ShapeDtypeStruct((rows, width), stream.dtype),
        in_specs=[vmem, vmem, vmem, vmem, vmem, vmem, vmem, hbm, hbm, hbm],
        out_specs=vmem,
        scratch_shapes=[
            pltpu.VMEM((rows, cols), jnp.bfloat16),
            pltpu.VMEM((SPAN + rows, cols), jnp.float32),
            pltpu.VMEM((SPAN, cols), jnp.bfloat16),
            pltpu.VMEM((SPAN, cols), jnp.bfloat16),
            pltpu.VMEM((8, rows), jnp.float32),
            pltpu.VMEM((levels, CORES * rows, width), jnp.bfloat16),
            pltpu.VMEM((sp_count, 8, rows), jnp.float32),
            pltpu.VMEM((sp_count, rows), jnp.float32),
            pltpu.VMEM((sp_count, rows), jnp.float32),
            pltpu.VMEM((pieces, width, 2 * LANES), jnp.bfloat16),
            pltpu.VMEM((hidden, width), jnp.bfloat16),
            pltpu.VMEM((CORES * slots, width), jnp.bfloat16),
            pltpu.VMEM((CORES * slots, hidden), jnp.bfloat16),
            pltpu.VMEM((CORES, rows, slots), jnp.bfloat16),
            pltpu.VMEM((CORES, slots, 1), jnp.float32),
            pltpu.VMEM((levels, CORES, rows, width), jnp.bfloat16),
            pltpu.VMEM((levels, rows, width), jnp.bfloat16),
            whole, halved, halved, whole, whole, whole, whole, whole, whole,
            pltpu.SemaphoreType.DMA((KINDS, max(2, levels))),
            pltpu.SemaphoreType.DMA((KINDS, max(2, levels))),
            pltpu.SemaphoreType.DMA((levels, tp_count)),
            pltpu.SemaphoreType.DMA((levels, tp_count)),
            pltpu.SemaphoreType.DMA((levels, tp_count)),
            pltpu.SemaphoreType.DMA((levels, tp_count)),
            pltpu.SemaphoreType.DMA((10, levels)),
            pltpu.SemaphoreType.DMA((6, levels)),
            pltpu.SemaphoreType.DMA((sp_count,)),
            pltpu.SemaphoreType.DMA((sp_count,)),
            pltpu.SemaphoreType.DMA((pieces + 1, 2)),
            pltpu.SemaphoreType.DMA((1,)),
            pltpu.SemaphoreType.DMA((1,)),
            pltpu.SemaphoreType.DMA((1,)),
        ],
        compiler_params=pltpu.CompilerParams(
            collective_id=0, has_side_effects=True, vmem_limit_bytes=62 * 1024 * 1024
        ),
        name="layer_all",
    )(stream, mix_gain, pool, pool_scale, ids, shares, gain, gate, up, down)


def shards(
    residual_in,
    mix_gain,
    pool_weight,
    pool_scale,
    ffn_gain,
    route_ids,
    route_weights,
    gate_weight,
    up_weight,
    down_weight,
):
    tp_count = lax.axis_size("tp")
    sp_count = lax.axis_size("sp")
    block_rows = residual_in.shape[0] // tp_count
    return layer_all(
        residual_in,
        mix_gain[None],
        pool_weight,
        pool_scale[None],
        route_ids.T,
        route_weights.T,
        ffn_gain[None],
        gate_weight,
        up_weight,
        down_weight,
        2 * TOP_K * block_rows // sp_count,
        sp_count,
        tp_count,
    )


def solution(mesh):
    placed = (
        P("sp", None),
        P(),
        P(None, "tp"),
        P("tp"),
        P(),
        P("sp", None),
        P("sp", None),
        P("sp", None, "tp"),
        P("sp", None, "tp"),
        P("sp", "tp", None),
    )
    square = mesh.shape["tp"] == SIDE * SIDE and mesh.shape["sp"] % CORES == 0
    return jax.shard_map(
        shards if square else shards_any,
        mesh=mesh,
        in_specs=placed,
        out_specs=P("sp", None),
        check_vma=False,
    )
```
